32 devices in a mesh: sp: 4 (over z), dp: 8 (over y, x, core).
Axes of the slice: x: 2, y: 2, z: 4, core: 2. Of those that a mesh axis runs over, the one named last changes fastest.
Arguments:
- inputs: bfloat16 [8, 512, 2048], P('dp', 'sp'), may hold values from -0.75 to 0.75
- queries: bfloat16 [8, 512, 1024], P('dp', 'sp'), may hold values from -18 to 18
- keys: bfloat16 [8, 512, 256], P('dp', 'sp'), may hold values from -18 to 18
- values: bfloat16 [8, 512, 256], P('dp', 'sp'), may hold values from -6 to 6
- out_grad: bfloat16 [8, 512, 1024], P('dp', 'sp'), may hold values from -144 to 144
- query_gain: float32 [64], replicated, may hold values from 0.4 to 6.5
- key_gain: float32 [64], replicated, may hold values from 0.4 to 6.5
- key_matrix: bfloat16 [2048, 256], P('dp'), may hold values from -0.125 to 0.125
- value_matrix: bfloat16 [2048, 256], P('dp'), may hold values from -0.125 to 0.125
Outputs:
- input_grad: bfloat16 [8, 512, 2048], P('dp', 'sp')
- query_grad: bfloat16 [8, 512, 1024], P('dp', 'sp')
- key_weight_grad: float32 [2048, 256], P('dp')
- value_weight_grad: float32 [2048, 256], P('dp')
The draws below stay inside these ranges and needn't reach their ends.
All inputs are finite; a program needn't handle non-finite values.
Results may differ from the reference program's by a relative error of at most 0.024.
The reference program's roundings to bfloat16 on the way count: a program that leaves them out, or rounds other values in their place, can miss the bound.
Values may be sent and summed in bfloat16 or wider, within the bound.
A program may use at most 64 MiB of HBM per device.

```python
import jax
import jax.numpy as jnp
from jax import lax

MODEL_WIDTH = 2048
QUERY_HEADS = 16
KEY_VALUE_HEADS = 4
HEAD_CHANNELS = 64
GRID = 64
SEQUENCE_LENGTH = 512
SEQUENCE_COUNT = 8
HPART = 4


def gain_draw(seed_key):
    return jnp.clip(1.0 + 0.18 * jax.random.normal(seed_key, (HEAD_CHANNELS,), jnp.float32), 0.4, 1.6)


def draw_query_gain(key, part):
    return gain_draw(jax.random.fold_in(key, 11))


def draw_key_gain(key, part):
    return gain_draw(jax.random.fold_in(key, 23))


def level_of(stream_key, extent, cuts, low, largest):
    def one(dim, parts):
        steps = jax.random.uniform(jax.random.fold_in(jax.random.fold_in(stream_key, 6), dim), (parts,), jnp.float32, low / len(cuts), largest / len(cuts))
        return jnp.repeat(jnp.exp(steps), extent[dim] // parts).reshape((-1,) + (1,) * (len(extent) - dim - 1))

    level = one(*cuts[0])
    for cut in cuts[1:]:
        level = level * one(*cut)
    return level


def bell_draw(rng, shape, deviation, limit, shards=(), kind=jnp.bfloat16):
    entries = jax.random.normal(rng, shape, jnp.float32) * deviation
    if len(shards) > 0:
        entries = level_of(rng, shape, shards, -0.22, 0.18) * entries
    return jnp.clip(entries, min=-limit, max=limit).astype(kind)


def setup_inputs(seed: int = 0) -> dict:
    arg_keys = jax.random.split(jax.random.key(seed), 10)
    return {
        "inputs": bell_draw(arg_keys[0], (SEQUENCE_COUNT, SEQUENCE_LENGTH, MODEL_WIDTH), 0.125, 0.75, ((0, 8), (1, 4))),
        "queries": bell_draw(arg_keys[1], (SEQUENCE_COUNT, SEQUENCE_LENGTH, QUERY_HEADS * HEAD_CHANNELS), 3.0, 18.0, ((0, 8), (1, 4))),
        "keys": bell_draw(arg_keys[2], (SEQUENCE_COUNT, SEQUENCE_LENGTH, KEY_VALUE_HEADS * HEAD_CHANNELS), 3.0, 18.0, ((0, 8), (1, 4))),
        "values": bell_draw(arg_keys[3], (SEQUENCE_COUNT, SEQUENCE_LENGTH, KEY_VALUE_HEADS * HEAD_CHANNELS), 1.0, 6.0, ((0, 8), (1, 4))),
        "out_grad": bell_draw(arg_keys[4], (SEQUENCE_COUNT, SEQUENCE_LENGTH, QUERY_HEADS * HEAD_CHANNELS), 24.0, 144.0, ((0, 8), (1, 4))),
        "query_gain": draw_query_gain(jax.random.fold_in(arg_keys[9], 71), 0),
        "key_gain": draw_key_gain(jax.random.fold_in(arg_keys[9], 71), 0),
        "key_matrix": bell_draw(arg_keys[7], (MODEL_WIDTH, KEY_VALUE_HEADS * HEAD_CHANNELS), MODEL_WIDTH ** -0.5, 0.125, ((0, 8),)),
        "value_matrix": bell_draw(arg_keys[8], (MODEL_WIDTH, KEY_VALUE_HEADS * HEAD_CHANNELS), MODEL_WIDTH ** -0.5, 0.125, ((0, 8),)),
    }


rope_base = 10000.0
norm_eps = 0.5
score_scale = 0.125

def product(pattern, first_op, second_op):
    return jnp.einsum(pattern, first_op.astype(jnp.float32), second_op.astype(jnp.float32))

def rotary_tables(token_length):
    position = jnp.arange(token_length, dtype=jnp.int32)
    grid_row = (position // GRID).astype(jnp.float32)
    grid_col = (position % GRID).astype(jnp.float32)
    half_pairs = HEAD_CHANNELS // 4
    inv_freq = rope_base ** (-jnp.arange(half_pairs, dtype=jnp.float32) / half_pairs)
    angles = jnp.concatenate([grid_row[:, None] * inv_freq, grid_col[:, None] * inv_freq], axis=1)
    return (jnp.cos(angles), jnp.sin(angles))

def rotate(vector, cos_tab, sin_tab):
    even_part = vector[..., 0::2]
    odd_part = vector[..., 1::2]
    turned = jnp.stack([even_part * cos_tab - odd_part * sin_tab, even_part * sin_tab + odd_part * cos_tab], axis=-1)
    return turned.reshape(vector.shape)

def rotate_back(cotangent, cos_tab, sin_tab):
    even_part = cotangent[..., 0::2]
    odd_part = cotangent[..., 1::2]
    turned = jnp.stack([even_part * cos_tab + odd_part * sin_tab, odd_part * cos_tab - even_part * sin_tab], axis=-1)
    return turned.reshape(cotangent.shape)

def inverse_rms(vector):
    return lax.rsqrt(lax.optimization_barrier(jnp.mean(vector * vector, axis=-1, keepdims=True)) + norm_eps)

def norm_back(vector, inv_scale, cotangent, gain_vec):
    weighted = cotangent * gain_vec
    inner_mean = lax.optimization_barrier(jnp.mean(weighted * vector, axis=-1, keepdims=True))
    return inv_scale * (weighted - vector * inv_scale * inv_scale * inner_mean)

def head_grads(query_in, key_input, value_input, grad_in, query_gain, key_gain, cos_tab, sin_tab, block_rows):
    token_length, groups, per_group, head_dim = query_in.shape
    cos_four = cos_tab[:, None, None, :]
    sin_four = sin_tab[:, None, None, :]
    cos_three = cos_tab[:, None, :]
    sin_three = sin_tab[:, None, :]
    query_f = query_in.astype(jnp.float32)
    query_inv = inverse_rms(query_f)
    query_rot = rotate(query_f * query_inv * query_gain, cos_four, sin_four).astype(jnp.bfloat16)
    key_f = key_input.astype(jnp.float32)
    key_inv = inverse_rms(key_f)
    key_rot = rotate(key_f * key_inv * key_gain, cos_three, sin_three).astype(jnp.bfloat16)
    num_blocks = token_length // block_rows
    query_blocks = query_rot.reshape(num_blocks, block_rows, groups, per_group, head_dim)
    grad_blocks = grad_in.reshape(num_blocks, block_rows, groups, per_group, head_dim)

    def attend_block(carried, pieces):
        key_acc, value_acc = carried
        query_piece, grad_piece = pieces
        scores = product('qgrd,cgd->grqc', query_piece, key_rot) * score_scale
        row_max = lax.optimization_barrier(jnp.max(scores, axis=-1, keepdims=True))
        shifted = jnp.exp(scores - row_max)
        attn_prob = shifted / lax.optimization_barrier(jnp.sum(shifted, axis=-1, keepdims=True))
        prob_low = attn_prob.astype(jnp.bfloat16)
        prob_grad = product('qgrd,cgd->grqc', grad_piece, value_input)
        row_dot = lax.optimization_barrier(jnp.sum(attn_prob * prob_grad, axis=-1, keepdims=True))
        score_grad = (attn_prob * (prob_grad - row_dot) * score_scale).astype(jnp.bfloat16)
        dq_piece = product('grqc,cgd->qgrd', score_grad, key_rot)
        key_acc = key_acc + product('grqc,qgrd->cgd', score_grad, query_piece)
        value_acc = value_acc + product('grqc,qgrd->cgd', prob_low, grad_piece)
        return ((key_acc, value_acc), dq_piece)
    empty_acc = jnp.zeros((token_length, groups, head_dim), jnp.float32)
    (key_rot_grad, value_acc), query_rot_grad = lax.scan(attend_block, (empty_acc, empty_acc), (query_blocks, grad_blocks))
    query_rot_grad = query_rot_grad.reshape(token_length, groups, per_group, head_dim)
    query_grad = norm_back(query_f, query_inv, rotate_back(query_rot_grad, cos_four, sin_four), query_gain).astype(jnp.bfloat16)
    key_portion = norm_back(key_f, key_inv, rotate_back(key_rot_grad, cos_three, sin_three), key_gain).astype(jnp.bfloat16)
    return (query_grad, key_portion, value_acc.astype(jnp.bfloat16))

def reference(inputs, queries, keys, values, out_grad, query_gain, key_gain, key_matrix, value_matrix):
    token_length = queries.shape[1]
    portion_count = QUERY_HEADS // HPART
    group_copies = portion_count // KEY_VALUE_HEADS
    cos_tab, sin_tab = rotary_tables(token_length)
    block_rows = min(512, token_length)

    def sequence_grads(pack):
        query_in, key_input, value_input, grad_in = pack
        key_positions = jnp.repeat(key_input.reshape(token_length, KEY_VALUE_HEADS, HEAD_CHANNELS), group_copies, axis=1)
        value_positions = jnp.repeat(value_input.reshape(token_length, KEY_VALUE_HEADS, HEAD_CHANNELS), group_copies, axis=1)
        query_part, key_portion, value_portion = head_grads(query_in.reshape(token_length, portion_count, HPART, HEAD_CHANNELS), key_positions, value_positions, grad_in.reshape(token_length, portion_count, HPART, HEAD_CHANNELS), query_gain, key_gain, cos_tab, sin_tab, block_rows)
        key_gradient = key_portion.reshape(token_length, KEY_VALUE_HEADS, group_copies, HEAD_CHANNELS).astype(jnp.float32).sum(axis=2).astype(jnp.bfloat16)
        value_gradient = value_portion.reshape(token_length, KEY_VALUE_HEADS, group_copies, HEAD_CHANNELS).astype(jnp.float32).sum(axis=2).astype(jnp.bfloat16)
        joined_output = jnp.concatenate([key_gradient.reshape(token_length, KEY_VALUE_HEADS * HEAD_CHANNELS), value_gradient.reshape(token_length, KEY_VALUE_HEADS * HEAD_CHANNELS)], axis=1)
        return (query_part.reshape(token_length, QUERY_HEADS * HEAD_CHANNELS), joined_output)
    query_grad, projection_gradient = lax.map(sequence_grads, (queries, keys, values, out_grad))
    joined_weight = jnp.concatenate([key_matrix, value_matrix], axis=1)
    flattened_gradient = projection_gradient.reshape(-1, 2 * KEY_VALUE_HEADS * HEAD_CHANNELS)
    input_grad = jnp.dot(flattened_gradient, joined_weight.T, preferred_element_type=jnp.float32).astype(jnp.bfloat16)
    input_grad = input_grad.reshape(inputs.shape)
    weight_grad = jnp.dot(inputs.reshape(-1, inputs.shape[2]).T, flattened_gradient, preferred_element_type=jnp.float32)
    key_value_width = KEY_VALUE_HEADS * HEAD_CHANNELS
    return (input_grad, query_grad, weight_grad[:, :key_value_width], weight_grad[:, key_value_width:])
```

```python
import functools

import jax
import jax.numpy as jnp
import numpy as np
from jax import lax
from jax.experimental import pallas as pl
from jax.experimental.pallas import tpu as pltpu
from jax.sharding import PartitionSpec as P

QUERY_HEADS = 16
KEY_VALUE_HEADS = 4
HEAD_CHANNELS = 64
GRID = 64


rope_base = 10000.0
norm_eps = 0.5
score_scale = 0.125


def product(pattern, first_op, second_op):
    return jnp.einsum(pattern, first_op, second_op, preferred_element_type=jnp.float32)


def rotary_tables(token_length):
    position = jnp.arange(token_length, dtype=jnp.int32)
    grid_row = (position // GRID).astype(jnp.float32)
    grid_col = (position % GRID).astype(jnp.float32)
    half_pairs = HEAD_CHANNELS // 4
    inv_freq = rope_base ** (-jnp.arange(half_pairs, dtype=jnp.float32) / half_pairs)
    angles = jnp.concatenate([grid_row[:, None] * inv_freq, grid_col[:, None] * inv_freq], axis=1)
    return (jnp.cos(angles), jnp.sin(angles))


def rotate(vector, cos_tab, sin_tab):
    even_part = vector[..., 0::2]
    odd_part = vector[..., 1::2]
    turned = jnp.stack(
        [even_part * cos_tab - odd_part * sin_tab, even_part * sin_tab + odd_part * cos_tab],
        axis=-1,
    )
    return turned.reshape(vector.shape)


def rotate_back(cotangent, cos_tab, sin_tab):
    even_part = cotangent[..., 0::2]
    odd_part = cotangent[..., 1::2]
    turned = jnp.stack(
        [even_part * cos_tab + odd_part * sin_tab, odd_part * cos_tab - even_part * sin_tab],
        axis=-1,
    )
    return turned.reshape(cotangent.shape)


def inverse_rms(vector):
    return lax.rsqrt(jnp.mean(vector * vector, axis=-1, keepdims=True) + norm_eps)


def norm_back(vector, inv_scale, cotangent, gain_vec):
    weighted = cotangent * gain_vec
    inner_mean = jnp.mean(weighted * vector, axis=-1, keepdims=True)
    return inv_scale * (weighted - vector * inv_scale * inv_scale * inner_mean)


def head_grads(
    query_in, key_input, value_input, grad_in, query_gain, key_gain, cos_tab, sin_tab, block_rows
):
    token_length, groups, per_group, head_dim = query_in.shape
    cos_four = cos_tab[:, None, None, :]
    sin_four = sin_tab[:, None, None, :]
    cos_three = cos_tab[:, None, :]
    sin_three = sin_tab[:, None, :]
    query_f = query_in.astype(jnp.float32)
    query_inv = inverse_rms(query_f)
    query_rot = rotate(query_f * query_inv * query_gain, cos_four, sin_four).astype(jnp.bfloat16)
    key_f = key_input.astype(jnp.float32)
    key_inv = inverse_rms(key_f)
    key_rot = rotate(key_f * key_inv * key_gain, cos_three, sin_three).astype(jnp.bfloat16)
    num_blocks = token_length // block_rows
    query_blocks = query_rot.reshape(num_blocks, block_rows, groups, per_group, head_dim)
    grad_blocks = grad_in.reshape(num_blocks, block_rows, groups, per_group, head_dim)

    def attend_block(carried, pieces):
        key_acc, value_acc = carried
        query_piece, grad_piece = pieces
        scores = product("qgrd,cgd->grqc", query_piece, key_rot) * score_scale
        row_max = jnp.max(scores, axis=-1, keepdims=True)
        shifted = jnp.exp(scores - row_max)
        attn_prob = shifted / jnp.sum(shifted, axis=-1, keepdims=True)
        prob_low = attn_prob.astype(jnp.bfloat16)
        prob_grad = product("qgrd,cgd->grqc", grad_piece, value_input)
        row_dot = jnp.sum(attn_prob * prob_grad, axis=-1, keepdims=True)
        score_grad = (attn_prob * (prob_grad - row_dot) * score_scale).astype(jnp.bfloat16)
        dq_piece = product("grqc,cgd->qgrd", score_grad, key_rot)
        key_acc = key_acc + product("grqc,qgrd->cgd", score_grad, query_piece)
        value_acc = value_acc + product("grqc,qgrd->cgd", prob_low, grad_piece)
        return ((key_acc, value_acc), dq_piece)

    empty_acc = jnp.zeros((token_length, groups, head_dim), jnp.float32)
    (key_rot_grad, value_acc), query_rot_grad = lax.scan(
        attend_block, (empty_acc, empty_acc), (query_blocks, grad_blocks)
    )
    query_rot_grad = query_rot_grad.reshape(token_length, groups, per_group, head_dim)
    query_grad = norm_back(
        query_f, query_inv, rotate_back(query_rot_grad, cos_four, sin_four), query_gain
    ).astype(jnp.bfloat16)
    key_portion = norm_back(
        key_f, key_inv, rotate_back(key_rot_grad, cos_three, sin_three), key_gain
    ).astype(jnp.bfloat16)
    return (query_grad, key_portion, value_acc.astype(jnp.bfloat16))


def on_device(
    inputs, queries, keys, values, out_grad, query_gain, key_gain, key_matrix, value_matrix
):
    sp_count = lax.axis_size("sp")
    dp_count = lax.axis_size("dp")
    token_row_block = inputs.shape[1]
    token_length = token_row_block * sp_count
    local_heads = QUERY_HEADS // sp_count
    portion_heads = min(local_heads, QUERY_HEADS // KEY_VALUE_HEADS)
    kv_here = local_heads // portion_heads
    group_copies = QUERY_HEADS // KEY_VALUE_HEADS // portion_heads
    key_value_width = KEY_VALUE_HEADS * HEAD_CHANNELS
    key_positions = jnp.repeat(
        keys[0].reshape(token_row_block, KEY_VALUE_HEADS, HEAD_CHANNELS), group_copies, axis=1
    ).reshape(token_row_block, key_value_width * group_copies)
    value_positions = jnp.repeat(
        values[0].reshape(token_row_block, KEY_VALUE_HEADS, HEAD_CHANNELS), group_copies, axis=1
    ).reshape(token_row_block, key_value_width * group_copies)
    grad_heads, query_heads, key_heads, value_heads = (
        lax.all_to_all(out_grad[0], "sp", split_axis=1, concat_axis=0, tiled=True),
        lax.all_to_all(queries[0], "sp", split_axis=1, concat_axis=0, tiled=True),
        lax.all_to_all(key_positions, "sp", split_axis=1, concat_axis=0, tiled=True),
        lax.all_to_all(value_positions, "sp", split_axis=1, concat_axis=0, tiled=True),
    )
    cos_tab, sin_tab = rotary_tables(token_length)
    query_part, key_portion, value_portion = head_grads(
        query_heads.reshape(token_length, kv_here, portion_heads, HEAD_CHANNELS),
        key_heads.reshape(token_length, kv_here, HEAD_CHANNELS),
        value_heads.reshape(token_length, kv_here, HEAD_CHANNELS),
        grad_heads.reshape(token_length, kv_here, portion_heads, HEAD_CHANNELS),
        query_gain,
        key_gain,
        cos_tab,
        sin_tab,
        min(512, token_length),
    )
    query_tokens, key_token_rows, value_token_rows = (
        lax.all_to_all(
            query_part.reshape(token_length, local_heads * HEAD_CHANNELS),
            "sp",
            split_axis=0,
            concat_axis=1,
            tiled=True,
        ),
        lax.all_to_all(
            key_portion.reshape(token_length, kv_here * HEAD_CHANNELS),
            "sp",
            split_axis=0,
            concat_axis=1,
            tiled=True,
        ),
        lax.all_to_all(
            value_portion.reshape(token_length, kv_here * HEAD_CHANNELS),
            "sp",
            split_axis=0,
            concat_axis=1,
            tiled=True,
        ),
    )
    key_gradient = (
        key_token_rows.reshape(token_row_block, KEY_VALUE_HEADS, group_copies, HEAD_CHANNELS)
        .astype(jnp.float32)
        .sum(axis=2)
        .astype(jnp.bfloat16)
    )
    value_gradient = (
        value_token_rows.reshape(token_row_block, KEY_VALUE_HEADS, group_copies, HEAD_CHANNELS)
        .astype(jnp.float32)
        .sum(axis=2)
        .astype(jnp.bfloat16)
    )
    projection_gradient = jnp.concatenate(
        [
            key_gradient.reshape(token_row_block, key_value_width),
            value_gradient.reshape(token_row_block, key_value_width),
        ],
        axis=1,
    )
    joined_weight = jnp.concatenate([key_matrix, value_matrix], axis=1)
    input_grad = lax.dot_general(
        projection_gradient,
        lax.all_gather(joined_weight, "dp", axis=0, tiled=True),
        (((1,), (1,)), ((), ())),
        preferred_element_type=jnp.float32,
    ).astype(jnp.bfloat16)
    token_in = inputs[0]
    width = inputs.shape[2]
    row_share = width // (sp_count * dp_count)
    permuted = (
        token_in.reshape(token_row_block, dp_count, sp_count, row_share)
        .transpose(0, 2, 1, 3)
        .reshape(token_row_block, width)
    )
    share_cols = lax.all_to_all(permuted, "sp", split_axis=1, concat_axis=0, tiled=True)
    all_grads = lax.all_gather(projection_gradient, "sp", axis=0, tiled=True)
    grad_piece = lax.psum_scatter(
        lax.dot_general(
            share_cols, all_grads, (((0,), (0,)), ((), ())), preferred_element_type=jnp.float32
        ).astype(jnp.bfloat16),
        "dp",
        scatter_dimension=0,
        tiled=True,
    ).astype(jnp.float32)
    weight_grad = lax.all_gather(grad_piece, "sp", axis=0, tiled=True)
    return (
        input_grad[None],
        query_tokens[None],
        weight_grad[:, :key_value_width],
        weight_grad[:, key_value_width:],
    )


LANES = 128
VMEM_BYTES = 67043328
MESH = pl.DeviceIdType.MESH
F32 = jnp.float32
BF16 = jnp.bfloat16


def pair_tables(token_length):
    position = np.arange(token_length)
    half_pairs = HEAD_CHANNELS // 4
    inv_freq = (rope_base ** (-np.arange(half_pairs) / half_pairs)).astype(np.float32)
    row = (position // GRID).astype(np.float32)
    col = (position % GRID).astype(np.float32)
    angles = np.concatenate([row[:, None] * inv_freq, col[:, None] * inv_freq], axis=1)
    cos_tab = np.repeat(np.cos(angles), 2, axis=1)
    sin_tab = np.repeat(np.sin(angles), 2, axis=1)
    sin_tab[:, 0::2] *= -1.0
    return (
        np.tile(cos_tab, (1, 2)).astype(np.float32),
        np.tile(sin_tab, (1, 2)).astype(np.float32),
    )


def swap_pairs(x):
    lane = lax.broadcasted_iota(jnp.int32, x.shape, 1)
    return jnp.where(lane % 2 == 0, pltpu.roll(x, LANES - 1, 1), pltpu.roll(x, 1, 1))


def head_mean(z):
    row = lax.broadcasted_iota(jnp.int32, (LANES, LANES), 0) // HEAD_CHANNELS
    col = lax.broadcasted_iota(jnp.int32, (LANES, LANES), 1) // HEAD_CHANNELS
    ones = jnp.where(row == col, 1.0, 0.0).astype(BF16)
    high = z.astype(BF16)
    low = (z - high.astype(F32)).astype(BF16)
    total = jnp.dot(high, ones, preferred_element_type=F32)
    total = total + jnp.dot(low, ones, preferred_element_type=F32)
    return total * (1.0 / HEAD_CHANNELS)


def norm_rotate(x, gain, cos_tab, sin_tab):
    inv = lax.rsqrt(head_mean(x * x) + norm_eps)
    y = x * inv * gain
    return y * cos_tab + swap_pairs(y) * sin_tab, inv


def norm_rotate_back(x, inv, cotangent, gain, cos_tab, sin_tab):
    turned = cotangent * cos_tab - swap_pairs(cotangent) * sin_tab
    weighted = turned * gain
    return inv * (weighted - x * (inv * inv * head_mean(weighted * x)))


def contract(a, b, dims):
    return lax.dot_general(a, b, (dims, ((), ())), preferred_element_type=F32)


def step_kernel(
    n, dp,
    x_hbm, q_hbm, k_hbm, v_hbm, do_hbm, qg_hbm, kg_hbm, km_hbm, vm_hbm, cos_hbm, sin_hbm,
    dx_buf, dq_buf, kw_buf, vw_buf,
    qg_ref, kg_ref, q_buf, do_buf, cos_buf, sin_buf, k_own, v_own, k_head, kv_all, q_inv, q_st, do_st,
    x_all, x_t, wk_all, wv_all, dq_acc, part, comb_in, comb, got, g_all, own_k, own_v,
    wg_part, wg_got, fin_all,
    local_sem, kv_send, kv_recv, x_sem, w_send, w_recv, p_send, c_recv, p_recv,
    g_send, gd_recv, gm_recv, r_send, r_recv, f_recv,
):
    me = lax.axis_index("sp")
    md = lax.axis_index("dp")
    rows, q_width = q_buf.shape
    heads = kv_all.shape[1]
    share = x_all.shape[2]
    per_group = q_width // (heads * HEAD_CHANNELS)
    half_share = share // 2
    mate = md + 1 - 2 * (md % 2)
    piece = share // n
    last = n - 1
    partner = me + 1 - 2 * (me % 2)
    low_side = me < n // 2
    other_end = jnp.where(low_side, last, 0)
    other_mid = jnp.where(low_side, n // 2, n // 2 - 1)
    is_end = jnp.logical_or(me == 0, me == last)
    near_chips = dp // 2 - 1

    def sp_peer(o):
        return lax.rem(me + o, n)

    def sp_from(o):
        return lax.rem(me - o + n, n)

    def dp_peer(o):
        return lax.rem(md + o, dp)

    def dp_from(o):
        return lax.rem(md - o + dp, dp)

    def mate_from(o):
        return lax.rem(mate - o + dp, dp)

    def pair(c):
        return pl.ds(c * LANES, LANES)

    def columns(d):
        return pl.ds(pl.multiple_of(d * share, share), share)

    barrier = pltpu.get_barrier_semaphore()

    def greet(where):
        pl.semaphore_signal(barrier, inc=1, device_id=where, device_id_type=MESH)

    @pl.when(me > 0)
    def _():
        greet({"sp": me - 1})

    @pl.when(me < last)
    def _():
        greet({"sp": me + 1})

    @pl.when(me == 0)
    def _():
        greet({"sp": last})

    for o in range(1, dp):
        greet({"dp": dp_peer(o)})

    my_rows = pl.ds(pl.multiple_of(me * rows, rows), rows)
    wanted = [
        (k_hbm, k_own), (v_hbm, v_own), (cos_hbm.at[my_rows, :], cos_buf),
        (sin_hbm.at[my_rows, :], sin_buf), (kg_hbm, kg_ref), (qg_hbm, qg_ref),
        (q_hbm, q_buf), (do_hbm, do_buf),
        (x_hbm.at[:, columns(md)], x_all.at[md]), (km_hbm, wk_all.at[md]), (vm_hbm, wv_all.at[md]),
    ]
    local = [
        pltpu.make_async_copy(src, dst, local_sem.at[i]) for i, (src, dst) in enumerate(wanted)
    ]
    for copy in local:
        copy.start()

    def remote(src, dst, send, recv, where):
        return pltpu.make_async_remote_copy(
            src_ref=src, dst_ref=dst, send_sem=send, recv_sem=recv,
            device_id=where, device_id_type=MESH,
        )

    def send(*args):
        remote(*args).start()

    def arrived(dst, recv):
        remote(dst, dst, recv, recv, {"sp": me}).wait_recv()

    def departed(src, sem):
        remote(src, src, sem, sem, {"sp": me}).wait_send()

    low_lanes = lax.broadcasted_iota(jnp.int32, (rows, LANES), 1) < HEAD_CHANNELS

    def shift(a):
        return pltpu.roll(a, HEAD_CHANNELS, 1)

    with jax.named_scope("local"):
        for copy in local[:6]:
            copy.wait()
    cos_own = cos_buf[...]
    sin_own = sin_buf[...]
    q_gain = jnp.concatenate([qg_ref[...], qg_ref[...]], axis=1)
    k_gain = jnp.concatenate([kg_ref[...], kg_ref[...]], axis=1)

    for c in range(heads // 2):
        keys = k_own[:, pair(c)].astype(F32)
        vals = v_own[:, pair(c)].astype(F32)
        turned = norm_rotate(keys, k_gain, cos_own, sin_own)[0]
        kv_all[me, 2 * c] = jnp.where(low_lanes, turned, shift(vals)).astype(BF16)
        kv_all[me, 2 * c + 1] = jnp.where(low_lanes, shift(turned), vals).astype(BF16)
        k_head[2 * c] = keys
        k_head[2 * c + 1] = shift(keys)

    with jax.named_scope("barrier"):
        pl.semaphore_wait(
            barrier, dp - 1 + jnp.where(me > 0, 1, 0) + jnp.where(me < last, 1, 0)
            + jnp.where(me == last, 1, 0)
        )

    def send_kv(src, g, sem, where):
        block = kv_all.at[src, g]
        send(block, block, kv_send.at[sem], kv_recv.at[src, g], {"sp": where})

    for g in range(heads):
        @pl.when(me < last)
        def _():
            send_kv(me, g, 0, me + 1)

        @pl.when(me > 0)
        def _():
            send_kv(me, g, 1, me - 1)

        @pl.when(me == last)
        def _():
            send_kv(me, g, 2, 0)

    for o in range(1, dp):
        send(x_hbm.at[:, columns(dp_peer(o))], x_all.at[md], x_sem.at[0], x_sem.at[1],
             {"dp": dp_peer(o)})

    top = pl.ds(0, half_share)
    bottom = pl.ds(half_share, half_share)
    full = pl.ds(0, share)
    weights = [(km_hbm, wk_all, full), (vm_hbm, wv_all, top), (vm_hbm, wv_all, bottom)]

    def send_weights(kind):
        src, dst, at = weights[kind]
        for o in range(2, dp, 2):
            send(src.at[at], dst.at[md, at], w_send.at[kind], w_recv.at[kind, 0],
                 {"dp": dp_peer(o)})
        send(src.at[at], dst.at[md, at], w_send.at[kind], w_recv.at[kind, 1], {"dp": mate})

    def pass_weights(kind):
        _, dst, at = weights[kind]
        arrived(dst.at[pl.ds(0, near_chips), at], w_recv.at[kind, 0])
        for o in range(2, dp, 2):
            block = dst.at[dp_from(o), at]
            send(block, block, w_send.at[kind], w_recv.at[kind, 1], {"dp": mate})

    def finish_weights(kind):
        _, dst, at = weights[kind]
        arrived(dst.at[pl.ds(0, dp // 2), at], w_recv.at[kind, 1])

    send_weights(0)
    send_weights(1)

    with jax.named_scope("local2"):
        for copy in local[6:8]:
            copy.wait()
    with jax.named_scope("qrot"):
        for c in range(q_width // LANES):
            turned, inv = norm_rotate(q_buf[:, pair(c)].astype(F32), q_gain, cos_own, sin_own)
            q_inv[:, pair(c)] = inv
            turned = turned * score_scale
            grads = do_buf[:, pair(c)].astype(F32)
            g, r = divmod(2 * c, per_group)
            for a, (query, grad) in enumerate([(turned, shift(grads)), (shift(turned), grads)]):
                to = pl.ds((r + a) * rows, rows)
                q_st[g, to, :] = jnp.where(low_lanes, query, 0.0).astype(BF16)
                do_st[g, to, :] = jnp.where(low_lanes, 0.0, grad).astype(BF16)

    def take_kv(src, g):
        arrived(kv_all.at[src, g], kv_recv.at[src, g])

    def relay(src, g, where):
        take_kv(src, g)
        send_kv(src, g, 3 + src, where)

    with jax.named_scope("relay"):
        @pl.when(me == 1)
        def _():
            for g in range(heads + 2):
                if g < heads:
                    relay(0, g, 2)
                if g >= 2:
                    relay(2, g - 2, 0)

        @pl.when(me == 2)
        def _():
            for g in range(heads):
                relay(1, g, 3)
                if g < 2:
                    relay(3, g, 1)
                relay(0, g, 3)

    def attend(g):
        kv = kv_all[:, g].reshape(n * rows, LANES)
        queries = q_st[g]
        grads = do_st[g]
        scores = contract(kv, queries, ((1,), (1,)))
        shifted = jnp.exp(scores - jnp.max(scores, axis=0, keepdims=True))
        prob = shifted * (1.0 / jnp.sum(shifted, axis=0, keepdims=True))
        prob_grad = contract(kv, grads, ((1,), (1,)))
        row_dot = jnp.sum(prob * prob_grad, axis=0, keepdims=True)
        score_grad = (prob * (prob_grad - row_dot)).astype(BF16)
        both = contract(score_grad, queries, ((1,), (0,)))
        both = both + contract(prob.astype(BF16), grads, ((1,), (0,)))
        part[g] = both.astype(BF16).reshape(n, rows, LANES)
        return kv, score_grad

    def query_part(g, kv, score_grad):
        dq_t = contract(kv[:, :HEAD_CHANNELS], score_grad, ((0,), (0,)))
        for r in range(0, per_group, 2):
            turned = jnp.concatenate(
                [dq_t[:, r * rows:(r + 1) * rows], dq_t[:, (r + 1) * rows:(r + 2) * rows]], axis=0
            )
            head = g * per_group + r
            dq_acc[:, head * HEAD_CHANNELS:head * HEAD_CHANNELS + LANES] = turned.T

    def send_parts(g):
        @pl.when(is_end)
        def _():
            send(part.at[g, other_end], comb_in.at[g, 0], p_send.at[0], c_recv.at[g, 0],
                 {"sp": partner})
            send(part.at[g, other_mid], comb_in.at[g, 1], p_send.at[0], c_recv.at[g, 1],
                 {"sp": partner})

        send(part.at[g, partner], got.at[g, 0], p_send.at[0], p_recv.at[g], {"sp": partner})

    def combine(g):
        @pl.when(jnp.logical_not(is_end))
        def _():
            for i, where in enumerate([other_end, other_mid]):
                arrived(comb_in.at[g, i], c_recv.at[g, i])
                total = comb_in[g, i].astype(F32) + part[g, where].astype(F32)
                comb[g, i] = total.astype(BF16)
                send(comb.at[g, i], got.at[g, 1], p_send.at[0], p_recv.at[g], {"sp": where})

    def own_grads(g):
        with jax.named_scope(f"gotwait{g}"):
            arrived(got.at[g], p_recv.at[g])
        total = part[g, me].astype(F32) + got[g, 0].astype(F32) + got[g, 1].astype(F32)
        keys = k_head[g]
        inv = lax.rsqrt(head_mean(keys * keys) + norm_eps)
        back = norm_rotate_back(keys, inv, total, k_gain, cos_own, sin_own)
        both = jnp.where(low_lanes, back, total).astype(BF16)
        g_all[g, md] = both
        mine = g_all.at[g, md]
        for o in range(2, dp, 2):
            send(mine, mine, g_send.at[0], gd_recv.at[g], {"dp": dp_peer(o)})
        send(mine, mine, g_send.at[0], gm_recv.at[g], {"dp": mate})
        at = slice(g * HEAD_CHANNELS, (g + 1) * HEAD_CHANNELS)
        own_k[:, at] = both[:, :HEAD_CHANNELS]
        own_v[:, at] = both[:, HEAD_CHANNELS:]

    def pass_on(g):
        with jax.named_scope(f"gdwait{g}"):
            arrived(g_all.at[g, pl.ds(0, near_chips)], gd_recv.at[g])
        for o in range(2, dp, 2):
            block = g_all.at[g, dp_from(o)]
            send(block, block, g_send.at[1], gm_recv.at[g], {"dp": mate})

    def weight_grads(g):
        with jax.named_scope(f"gmwait{g}"):
            arrived(g_all.at[g, pl.ds(0, dp // 2)], gm_recv.at[g])
        total = contract(x_t[...], g_all[g].reshape(dp * rows, LANES), ((1,), (0,)))
        wg_part[g] = total.astype(BF16).reshape(n, piece, LANES)
        for o in range(1, n):
            send(wg_part.at[g, sp_peer(o)], wg_got.at[g, me], r_send.at[0], r_recv.at[g],
                 {"sp": sp_peer(o)})

    def sum_weight_grads(g):
        with jax.named_scope(f"rwait{g}"):
            arrived(wg_got.at[g, pl.ds(0, last)], r_recv.at[g])
        total = wg_part[g, me].astype(F32)
        for o in range(1, n):
            total = total + wg_got[g, sp_from(o)].astype(F32)
        fin_all[g, me] = total.astype(BF16)
        mine = fin_all.at[g, me]
        for o in range(1, n):
            send(mine, mine, r_send.at[1], f_recv.at[g], {"sp": sp_peer(o)})

    def put_weight_grads(g):
        with jax.named_scope(f"fwait{g}"):
            arrived(fin_all.at[g, pl.ds(0, last)], f_recv.at[g])
        total = fin_all[g].reshape(share, LANES).astype(F32)
        at = slice(g * HEAD_CHANNELS, (g + 1) * HEAD_CHANNELS)
        kw_buf[:, at] = total[:, :HEAD_CHANNELS]
        vw_buf[:, at] = total[:, HEAD_CHANNELS:]

    def query_grads(c):
        dq_buf[:, pair(c)] = norm_rotate_back(
            q_buf[:, pair(c)].astype(F32), q_inv[:, pair(c)], dq_acc[:, pair(c)],
            q_gain * score_scale, cos_own, sin_own,
        ).astype(BF16)

    def project(src):
        out = contract(own_k[...], wk_all[src], ((1,), (1,)))
        out = out + contract(own_v[...], wv_all[src], ((1,), (1,)))
        dx_buf[:, columns(src)] = out.astype(BF16)

    blocks = q_width // LANES
    for g in range(heads):
        with jax.named_scope(f"kvwait{g}"):
            for role, sources in ((0, (1, 2, 3)), (1, (3,)), (3, (2, 1, 0))):
                @pl.when(me == role)
                def _():
                    for src in sources:
                        take_kv(src, g)
        with jax.named_scope(f"attend{g}"):
            kept = attend(g)
            send_parts(g)
            query_part(g, *kept)
        if g == 0:
            @pl.when(me == 2)
            def _():
                for k in range(2, heads):
                    relay(3, k, 1)
        if g == 2:
            with jax.named_scope("comb0"):
                combine(0)
    with jax.named_scope("comb1"):
        combine(1)
    with jax.named_scope("xt"):
        for copy in local[8:]:
            copy.wait()
        arrived(x_all.at[pl.ds(0, dp - 1)], x_sem.at[1])
        for src in range(dp):
            x_t[:, src * rows:(src + 1) * rows] = x_all[src].T
    with jax.named_scope("comb2"):
        combine(2)
    with jax.named_scope("dqa"):
        for c in range(blocks // 2):
            query_grads(c)
    with jax.named_scope("comb3"):
        combine(3)
    for g in range(heads):
        with jax.named_scope(f"own{g}"):
            own_grads(g)
    send_weights(2)
    with jax.named_scope("dqb"):
        for c in range(blocks // 2, blocks):
            query_grads(c)
    with jax.named_scope("wpass"):
        pass_weights(0)
        pass_weights(1)
    pass_on(0)
    pass_on(1)
    for g in range(heads):
        if g + 2 < heads:
            pass_on(g + 2)
        with jax.named_scope(f"wg{g}"):
            weight_grads(g)
    with jax.named_scope("sum0"):
        sum_weight_grads(0)
    with jax.named_scope("wlate"):
        pass_weights(2)
    sum_weight_grads(1)
    with jax.named_scope("proja"):
        for o in range(0, dp, 2):
            project(dp_from(o))
    sum_weight_grads(2)
    sum_weight_grads(3)
    with jax.named_scope("wfin"):
        for kind in range(3):
            finish_weights(kind)
    with jax.named_scope("projb"):
        for o in range(0, dp, 2):
            project(mate_from(o))
    for g in range(heads):
        with jax.named_scope(f"put{g}"):
            put_weight_grads(g)

    with jax.named_scope("drain"):
        @pl.when(me < last)
        def _():
            departed(kv_all.at[me], kv_send.at[0])

        @pl.when(me > 0)
        def _():
            departed(kv_all.at[me], kv_send.at[1])

        @pl.when(me == last)
        def _():
            departed(kv_all.at[me], kv_send.at[2])

        for role, sources in ((1, (0, 2)), (2, (0, 1, 3))):
            @pl.when(me == role)
            def _():
                for src in sources:
                    departed(kv_all.at[src], kv_send.at[3 + src])

        departed(x_all.at[pl.ds(0, dp - 1)], x_sem.at[0])
        for kind, (_, dst, at) in enumerate(weights):
            departed(dst.at[pl.ds(0, dp - 1), at], w_send.at[kind])
        departed(part.at[:, pl.ds(0, 3)], p_send.at[0])
        departed(g_all.at[:, pl.ds(0, dp // 2)], g_send.at[0])
        departed(g_all.at[:, pl.ds(0, near_chips)], g_send.at[1])
        departed(wg_part.at[:, pl.ds(0, last)], r_send.at[0])
        departed(fin_all.at[:, pl.ds(0, last)], r_send.at[1])


def write_kernel(*refs):
    count = (len(refs) - 1) // 2
    copies = [
        pltpu.make_async_copy(refs[i], refs[count + i], refs[-1].at[i]) for i in range(count)
    ]
    for copy in copies:
        copy.start()
    for copy in copies:
        copy.wait()


def kernel_step(
    n, dp, inputs, queries, keys, values, out_grad, query_gain, key_gain, key_matrix, value_matrix
):
    rows, width = inputs.shape[1:]
    q_width = queries.shape[2]
    kv_width = keys.shape[2]
    length = rows * n
    share = width // dp
    kv_heads = kv_width // HEAD_CHANNELS
    stack = rows * (q_width // kv_width)
    cos_tab, sin_tab = pair_tables(length)
    vmem = pltpu.VMEM
    dma = pltpu.SemaphoreType.DMA
    packed = (rows, LANES)
    scratch = [
        vmem((1, HEAD_CHANNELS), F32), vmem((1, HEAD_CHANNELS), F32),
        vmem((rows, q_width), BF16), vmem((rows, q_width), BF16),
        vmem(packed, F32), vmem(packed, F32),
        vmem((rows, kv_width), BF16), vmem((rows, kv_width), BF16),
        vmem((kv_heads, *packed), F32), vmem((n, kv_heads, *packed), BF16),
        vmem((rows, q_width), F32),
        vmem((kv_heads, stack, LANES), BF16), vmem((kv_heads, stack, LANES), BF16),
        vmem((dp, rows, share), BF16), vmem((share, dp * rows), BF16),
        vmem((dp, share, kv_width), BF16), vmem((dp, share, kv_width), BF16),
        vmem((rows, q_width), F32),
        vmem((kv_heads, n, *packed), BF16),
        vmem((kv_heads, 2, *packed), BF16), vmem((kv_heads, 2, *packed), BF16),
        vmem((kv_heads, 2, *packed), BF16),
        vmem((kv_heads, dp, *packed), BF16),
        vmem((rows, kv_width), BF16), vmem((rows, kv_width), BF16),
        vmem((kv_heads, n, share // n, LANES), BF16),
        vmem((kv_heads, n, share // n, LANES), BF16),
        vmem((kv_heads, n, share // n, LANES), BF16),
        dma((11,)), dma((3 + n,)), dma((n, kv_heads)), dma((2,)), dma((3,)), dma((3, 2)),
        dma((1,)), dma((kv_heads, 2)), dma((kv_heads,)),
        dma((2,)), dma((kv_heads,)), dma((kv_heads,)), dma((2,)), dma((kv_heads,)), dma((kv_heads,)),
    ]
    hbm = pl.BlockSpec(memory_space=pltpu.HBM)
    here = pl.BlockSpec(memory_space=pltpu.VMEM)
    results = [
        ((rows, width), BF16), ((rows, q_width), BF16),
        ((share, kv_width), F32), ((share, kv_width), F32),
    ]
    held_bytes = 65536 + sum(a * b * jnp.dtype(kind).itemsize for (a, b), kind in results)
    held = pl.pallas_call(
        functools.partial(step_kernel, n, dp),
        out_shape=[pltpu.VMEM(shape, kind) for shape, kind in results],
        in_specs=[hbm] * 11,
        out_specs=[here] * 4,
        scratch_shapes=scratch,
        compiler_params=pltpu.CompilerParams(
            collective_id=0, has_side_effects=True, vmem_limit_bytes=VMEM_BYTES - held_bytes
        ),
    )(
        inputs[0], queries[0], keys[0], values[0], out_grad[0],
        query_gain[None], key_gain[None],
        key_matrix, value_matrix, jnp.asarray(cos_tab), jnp.asarray(sin_tab),
    )
    dx, dq, kw, vw = pl.pallas_call(
        write_kernel,
        out_shape=[jax.ShapeDtypeStruct(shape, kind) for shape, kind in results],
        in_specs=[here] * 4,
        out_specs=[hbm] * 4,
        scratch_shapes=[dma((4,))],
        compiler_params=pltpu.CompilerParams(vmem_limit_bytes=8 * 1024 * 1024),
    )(*held)
    return dx[None], dq[None], kw, vw


def device_step(inputs, *rest):
    n = lax.axis_size("sp")
    dp = lax.axis_size("dp")
    rows, width = inputs.shape[1:]
    fits = n == 4 and dp == 8 and width % (dp * LANES) == 0 and rows == LANES
    if fits and (width // dp) % (32 * n) == 0:
        return kernel_step(n, dp, inputs, *rest)
    return on_device(inputs, *rest)


def solution(mesh):
    return jax.shard_map(
        device_step,
        mesh=mesh,
        in_specs=(
            P("dp", "sp", None),
            P("dp", "sp", None),
            P("dp", "sp", None),
            P("dp", "sp", None),
            P("dp", "sp", None),
            P(),
            P(),
            P("dp", None),
            P("dp", None),
        ),
        out_specs=(P("dp", "sp", None), P("dp", "sp", None), P("dp", None), P("dp", None)),
        check_vma=False,
    )
```

```python
import functools

import jax
import jax.numpy as jnp
import numpy as np
from jax import lax
from jax.experimental import pallas as pl
from jax.experimental.pallas import tpu as pltpu
from jax.sharding import PartitionSpec as P

QUERY_HEADS = 16
KEY_VALUE_HEADS = 4
HEAD_CHANNELS = 64
GRID = 64


rope_base = 10000.0
norm_eps = 0.5
score_scale = 0.125


def product(pattern, first_op, second_op):
    return jnp.einsum(pattern, first_op, second_op, preferred_element_type=jnp.float32)


def rotary_tables(token_length):
    position = jnp.arange(token_length, dtype=jnp.int32)
    grid_row = (position // GRID).astype(jnp.float32)
    grid_col = (position % GRID).astype(jnp.float32)
    half_pairs = HEAD_CHANNELS // 4
    inv_freq = rope_base ** (-jnp.arange(half_pairs, dtype=jnp.float32) / half_pairs)
    angles = jnp.concatenate([grid_row[:, None] * inv_freq, grid_col[:, None] * inv_freq], axis=1)
    return (jnp.cos(angles), jnp.sin(angles))


def rotate(vector, cos_tab, sin_tab):
    even_part = vector[..., 0::2]
    odd_part = vector[..., 1::2]
    turned = jnp.stack(
        [even_part * cos_tab - odd_part * sin_tab, even_part * sin_tab + odd_part * cos_tab],
        axis=-1,
    )
    return turned.reshape(vector.shape)


def rotate_back(cotangent, cos_tab, sin_tab):
    even_part = cotangent[..., 0::2]
    odd_part = cotangent[..., 1::2]
    turned = jnp.stack(
        [even_part * cos_tab + odd_part * sin_tab, odd_part * cos_tab - even_part * sin_tab],
        axis=-1,
    )
    return turned.reshape(cotangent.shape)


def inverse_rms(vector):
    return lax.rsqrt(jnp.mean(vector * vector, axis=-1, keepdims=True) + norm_eps)


def norm_back(vector, inv_scale, cotangent, gain_vec):
    weighted = cotangent * gain_vec
    inner_mean = jnp.mean(weighted * vector, axis=-1, keepdims=True)
    return inv_scale * (weighted - vector * inv_scale * inv_scale * inner_mean)


def head_grads(
    query_in, key_input, value_input, grad_in, query_gain, key_gain, cos_tab, sin_tab, block_rows
):
    token_length, groups, per_group, head_dim = query_in.shape
    cos_four = cos_tab[:, None, None, :]
    sin_four = sin_tab[:, None, None, :]
    cos_three = cos_tab[:, None, :]
    sin_three = sin_tab[:, None, :]
    query_f = query_in.astype(jnp.float32)
    query_inv = inverse_rms(query_f)
    query_rot = rotate(query_f * query_inv * query_gain, cos_four, sin_four).astype(jnp.bfloat16)
    key_f = key_input.astype(jnp.float32)
    key_inv = inverse_rms(key_f)
    key_rot = rotate(key_f * key_inv * key_gain, cos_three, sin_three).astype(jnp.bfloat16)
    num_blocks = token_length // block_rows
    query_blocks = query_rot.reshape(num_blocks, block_rows, groups, per_group, head_dim)
    grad_blocks = grad_in.reshape(num_blocks, block_rows, groups, per_group, head_dim)

    def attend_block(carried, pieces):
        key_acc, value_acc = carried
        query_piece, grad_piece = pieces
        scores = product("qgrd,cgd->grqc", query_piece, key_rot) * score_scale
        row_max = jnp.max(scores, axis=-1, keepdims=True)
        shifted = jnp.exp(scores - row_max)
        attn_prob = shifted / jnp.sum(shifted, axis=-1, keepdims=True)
        prob_low = attn_prob.astype(jnp.bfloat16)
        prob_grad = product("qgrd,cgd->grqc", grad_piece, value_input)
        row_dot = jnp.sum(attn_prob * prob_grad, axis=-1, keepdims=True)
        score_grad = (attn_prob * (prob_grad - row_dot) * score_scale).astype(jnp.bfloat16)
        dq_piece = product("grqc,cgd->qgrd", score_grad, key_rot)
        key_acc = key_acc + product("grqc,qgrd->cgd", score_grad, query_piece)
        value_acc = value_acc + product("grqc,qgrd->cgd", prob_low, grad_piece)
        return ((key_acc, value_acc), dq_piece)

    empty_acc = jnp.zeros((token_length, groups, head_dim), jnp.float32)
    (key_rot_grad, value_acc), query_rot_grad = lax.scan(
        attend_block, (empty_acc, empty_acc), (query_blocks, grad_blocks)
    )
    query_rot_grad = query_rot_grad.reshape(token_length, groups, per_group, head_dim)
    query_grad = norm_back(
        query_f, query_inv, rotate_back(query_rot_grad, cos_four, sin_four), query_gain
    ).astype(jnp.bfloat16)
    key_portion = norm_back(
        key_f, key_inv, rotate_back(key_rot_grad, cos_three, sin_three), key_gain
    ).astype(jnp.bfloat16)
    return (query_grad, key_portion, value_acc.astype(jnp.bfloat16))


def on_device(
    inputs, queries, keys, values, out_grad, query_gain, key_gain, key_matrix, value_matrix
):
    sp_count = lax.axis_size("sp")
    dp_count = lax.axis_size("dp")
    token_row_block = inputs.shape[1]
    token_length = token_row_block * sp_count
    local_heads = QUERY_HEADS // sp_count
    portion_heads = min(local_heads, QUERY_HEADS // KEY_VALUE_HEADS)
    kv_here = local_heads // portion_heads
    group_copies = QUERY_HEADS // KEY_VALUE_HEADS // portion_heads
    key_value_width = KEY_VALUE_HEADS * HEAD_CHANNELS
    key_positions = jnp.repeat(
        keys[0].reshape(token_row_block, KEY_VALUE_HEADS, HEAD_CHANNELS), group_copies, axis=1
    ).reshape(token_row_block, key_value_width * group_copies)
    value_positions = jnp.repeat(
        values[0].reshape(token_row_block, KEY_VALUE_HEADS, HEAD_CHANNELS), group_copies, axis=1
    ).reshape(token_row_block, key_value_width * group_copies)
    grad_heads, query_heads, key_heads, value_heads = (
        lax.all_to_all(out_grad[0], "sp", split_axis=1, concat_axis=0, tiled=True),
        lax.all_to_all(queries[0], "sp", split_axis=1, concat_axis=0, tiled=True),
        lax.all_to_all(key_positions, "sp", split_axis=1, concat_axis=0, tiled=True),
        lax.all_to_all(value_positions, "sp", split_axis=1, concat_axis=0, tiled=True),
    )
    cos_tab, sin_tab = rotary_tables(token_length)
    query_part, key_portion, value_portion = head_grads(
        query_heads.reshape(token_length, kv_here, portion_heads, HEAD_CHANNELS),
        key_heads.reshape(token_length, kv_here, HEAD_CHANNELS),
        value_heads.reshape(token_length, kv_here, HEAD_CHANNELS),
        grad_heads.reshape(token_length, kv_here, portion_heads, HEAD_CHANNELS),
        query_gain,
        key_gain,
        cos_tab,
        sin_tab,
        min(512, token_length),
    )
    query_tokens, key_token_rows, value_token_rows = (
        lax.all_to_all(
            query_part.reshape(token_length, local_heads * HEAD_CHANNELS),
            "sp",
            split_axis=0,
            concat_axis=1,
            tiled=True,
        ),
        lax.all_to_all(
            key_portion.reshape(token_length, kv_here * HEAD_CHANNELS),
            "sp",
            split_axis=0,
            concat_axis=1,
            tiled=True,
        ),
        lax.all_to_all(
            value_portion.reshape(token_length, kv_here * HEAD_CHANNELS),
            "sp",
            split_axis=0,
            concat_axis=1,
            tiled=True,
        ),
    )
    key_gradient = (
        key_token_rows.reshape(token_row_block, KEY_VALUE_HEADS, group_copies, HEAD_CHANNELS)
        .astype(jnp.float32)
        .sum(axis=2)
        .astype(jnp.bfloat16)
    )
    value_gradient = (
        value_token_rows.reshape(token_row_block, KEY_VALUE_HEADS, group_copies, HEAD_CHANNELS)
        .astype(jnp.float32)
        .sum(axis=2)
        .astype(jnp.bfloat16)
    )
    projection_gradient = jnp.concatenate(
        [
            key_gradient.reshape(token_row_block, key_value_width),
            value_gradient.reshape(token_row_block, key_value_width),
        ],
        axis=1,
    )
    joined_weight = jnp.concatenate([key_matrix, value_matrix], axis=1)
    input_grad = lax.dot_general(
        projection_gradient,
        lax.all_gather(joined_weight, "dp", axis=0, tiled=True),
        (((1,), (1,)), ((), ())),
        preferred_element_type=jnp.float32,
    ).astype(jnp.bfloat16)
    token_in = inputs[0]
    width = inputs.shape[2]
    row_share = width // (sp_count * dp_count)
    permuted = (
        token_in.reshape(token_row_block, dp_count, sp_count, row_share)
        .transpose(0, 2, 1, 3)
        .reshape(token_row_block, width)
    )
    share_cols = lax.all_to_all(permuted, "sp", split_axis=1, concat_axis=0, tiled=True)
    all_grads = lax.all_gather(projection_gradient, "sp", axis=0, tiled=True)
    grad_piece = lax.psum_scatter(
        lax.dot_general(
            share_cols, all_grads, (((0,), (0,)), ((), ())), preferred_element_type=jnp.float32
        ).astype(jnp.bfloat16),
        "dp",
        scatter_dimension=0,
        tiled=True,
    ).astype(jnp.float32)
    weight_grad = lax.all_gather(grad_piece, "sp", axis=0, tiled=True)
    return (
        input_grad[None],
        query_tokens[None],
        weight_grad[:, :key_value_width],
        weight_grad[:, key_value_width:],
    )


LANES = 128
VMEM_BYTES = 67043328
MESH = pl.DeviceIdType.MESH
F32 = jnp.float32
BF16 = jnp.bfloat16


def pair_tables(token_length):
    position = np.arange(token_length)
    half_pairs = HEAD_CHANNELS // 4
    inv_freq = (rope_base ** (-np.arange(half_pairs) / half_pairs)).astype(np.float32)
    row = (position // GRID).astype(np.float32)
    col = (position % GRID).astype(np.float32)
    angles = np.concatenate([row[:, None] * inv_freq, col[:, None] * inv_freq], axis=1)
    cos_tab = np.repeat(np.cos(angles), 2, axis=1)
    sin_tab = np.repeat(np.sin(angles), 2, axis=1)
    sin_tab[:, 0::2] *= -1.0
    return (
        np.tile(cos_tab, (1, 2)).astype(np.float32),
        np.tile(sin_tab, (1, 2)).astype(np.float32),
    )


def swap_pairs(x):
    lane = lax.broadcasted_iota(jnp.int32, x.shape, 1)
    return jnp.where(lane % 2 == 0, pltpu.roll(x, LANES - 1, 1), pltpu.roll(x, 1, 1))


def head_mean(z):
    row = lax.broadcasted_iota(jnp.int32, (LANES, LANES), 0) // HEAD_CHANNELS
    col = lax.broadcasted_iota(jnp.int32, (LANES, LANES), 1) // HEAD_CHANNELS
    ones = jnp.where(row == col, 1.0, 0.0).astype(BF16)
    high = z.astype(BF16)
    low = (z - high.astype(F32)).astype(BF16)
    total = jnp.dot(high, ones, preferred_element_type=F32)
    total = total + jnp.dot(low, ones, preferred_element_type=F32)
    return total * (1.0 / HEAD_CHANNELS)


def norm_rotate(x, gain, cos_tab, sin_tab):
    inv = lax.rsqrt(head_mean(x * x) + norm_eps)
    y = x * inv * gain
    return y * cos_tab + swap_pairs(y) * sin_tab, inv


def norm_rotate_back(x, inv, cotangent, gain, cos_tab, sin_tab):
    turned = cotangent * cos_tab - swap_pairs(cotangent) * sin_tab
    weighted = turned * gain
    return inv * (weighted - x * (inv * inv * head_mean(weighted * x)))


def contract(a, b, dims):
    return lax.dot_general(a, b, (dims, ((), ())), preferred_element_type=F32)


def step_kernel(
    n, dp,
    x_hbm, q_hbm, k_hbm, v_hbm, do_hbm, qg_hbm, kg_hbm, km_hbm, vm_hbm, cos_hbm, sin_hbm,
    dx_buf, dq_buf, kw_buf, vw_buf,
    qg_ref, kg_ref, q_buf, do_buf, cos_buf, sin_buf, k_own, v_own, k_head, kv_all, q_inv, q_st, do_st,
    x_all, x_t, wk_all, wv_all, dq_acc, part, comb_in, comb, got, g_all, own_k, own_v,
    wg_part, wg_got, fin_all, fin_low,
    local_sem, kv_send, kv_recv, x_sem, w_send, w_recv, p_send, c_recv, p_recv,
    g_send, gd_recv, gm_recv, r_send, r_recv, f_recv,
):
    me = lax.axis_index("sp")
    md = lax.axis_index("dp")
    rows, q_width = q_buf.shape
    heads = kv_all.shape[1]
    share = x_all.shape[2]
    per_group = q_width // (heads * HEAD_CHANNELS)
    half_share = share // 2
    mate = md + 1 - 2 * (md % 2)
    last = n - 1
    first_mid = n // 2 - 1
    partner = me + 1 - 2 * (me % 2)
    low_side = me < n // 2
    other_end = jnp.where(low_side, last, 0)
    other_mid = jnp.where(low_side, n // 2, n // 2 - 1)
    is_end = jnp.logical_or(me == 0, me == last)
    near_chips = dp // 2 - 1
    core = md % 2
    upper = md + 1 - core
    side_mid = jnp.where(is_end, partner, me)
    is_owner = jnp.logical_and(jnp.logical_not(is_end), core == 1)
    relayed = 1

    def sp_peer(o):
        return lax.rem(me + o, n)

    def sp_from(o):
        return lax.rem(me - o + n, n)

    def dp_peer(o):
        return lax.rem(md + o, dp)

    def dp_from(o):
        return lax.rem(md - o + dp, dp)

    def mate_from(o):
        return lax.rem(mate - o + dp, dp)

    def pair(c):
        return pl.ds(c * LANES, LANES)

    def columns(d):
        return pl.ds(pl.multiple_of(d * share, share), share)

    barrier = pltpu.get_barrier_semaphore()

    def greet(where):
        pl.semaphore_signal(barrier, inc=1, device_id=where, device_id_type=MESH)

    @pl.when(me > 0)
    def _():
        greet({"sp": me - 1})

    @pl.when(me < last)
    def _():
        greet({"sp": me + 1})

    @pl.when(jnp.logical_not(is_end))
    def _():
        greet({"sp": other_end})

    for o in range(1, dp):
        greet({"dp": dp_peer(o)})

    my_rows = pl.ds(pl.multiple_of(me * rows, rows), rows)
    wanted = [
        (k_hbm, k_own), (v_hbm, v_own), (cos_hbm.at[my_rows, :], cos_buf),
        (sin_hbm.at[my_rows, :], sin_buf), (kg_hbm, kg_ref), (qg_hbm, qg_ref),
        (q_hbm, q_buf), (do_hbm, do_buf),
        (x_hbm.at[:, columns(md)], x_all.at[md]), (km_hbm, wk_all.at[md]), (vm_hbm, wv_all.at[md]),
    ]
    local = [
        pltpu.make_async_copy(src, dst, local_sem.at[i]) for i, (src, dst) in enumerate(wanted)
    ]
    for copy in local:
        copy.start()

    def remote(src, dst, send, recv, where):
        return pltpu.make_async_remote_copy(
            src_ref=src, dst_ref=dst, send_sem=send, recv_sem=recv,
            device_id=where, device_id_type=MESH,
        )

    def send(*args):
        remote(*args).start()

    def arrived(dst, recv):
        remote(dst, dst, recv, recv, {"sp": me}).wait_recv()

    def departed(src, sem):
        remote(src, src, sem, sem, {"sp": me}).wait_send()

    low_lanes = lax.broadcasted_iota(jnp.int32, (rows, LANES), 1) < HEAD_CHANNELS

    def shift(a):
        return pltpu.roll(a, HEAD_CHANNELS, 1)

    with jax.named_scope("local"):
        for copy in local[:6]:
            copy.wait()
    cos_own = cos_buf[...]
    sin_own = sin_buf[...]
    q_gain = jnp.concatenate([qg_ref[...], qg_ref[...]], axis=1)
    k_gain = jnp.concatenate([kg_ref[...], kg_ref[...]], axis=1)

    for c in range(heads // 2):
        keys = k_own[:, pair(c)].astype(F32)
        vals = v_own[:, pair(c)].astype(F32)
        turned = norm_rotate(keys, k_gain, cos_own, sin_own)[0]
        kv_all[me, 2 * c] = jnp.where(low_lanes, turned, shift(vals)).astype(BF16)
        kv_all[me, 2 * c + 1] = jnp.where(low_lanes, shift(turned), vals).astype(BF16)
        k_head[2 * c] = keys
        k_head[2 * c + 1] = shift(keys)

    with jax.named_scope("barrier"):
        pl.semaphore_wait(barrier, dp + 1)

    def send_kv(src, g, sem, where):
        block = kv_all.at[src, g]
        send(block, block, kv_send.at[sem], kv_recv.at[src, g], {"sp": where})

    for g in range(heads):
        send_kv(me, g, 0, other_mid)
        send_kv(me, g, 1, partner)

    for o in range(1, dp):
        send(x_hbm.at[:, columns(dp_peer(o))], x_all.at[md], x_sem.at[0], x_sem.at[1],
             {"dp": dp_peer(o)})

    top = pl.ds(0, half_share)
    bottom = pl.ds(half_share, half_share)
    full = pl.ds(0, share)
    weights = [(km_hbm, wk_all, full), (vm_hbm, wv_all, top), (vm_hbm, wv_all, bottom)]

    def send_weights(kind):
        src, dst, at = weights[kind]
        for o in range(2, dp, 2):
            send(src.at[at], dst.at[md, at], w_send.at[kind], w_recv.at[kind, 0],
                 {"dp": dp_peer(o)})
        send(src.at[at], dst.at[md, at], w_send.at[kind], w_recv.at[kind, 1], {"dp": mate})

    def pass_weights(kind):
        _, dst, at = weights[kind]
        arrived(dst.at[pl.ds(0, near_chips), at], w_recv.at[kind, 0])
        for o in range(2, dp, 2):
            block = dst.at[dp_from(o), at]
            send(block, block, w_send.at[kind], w_recv.at[kind, 1], {"dp": mate})

    def finish_weights(kind):
        _, dst, at = weights[kind]
        arrived(dst.at[pl.ds(0, dp // 2), at], w_recv.at[kind, 1])

    send_weights(0)
    send_weights(1)

    with jax.named_scope("local2"):
        for copy in local[6:8]:
            copy.wait()
    with jax.named_scope("qrot"):
        for c in range(q_width // LANES):
            turned, inv = norm_rotate(q_buf[:, pair(c)].astype(F32), q_gain, cos_own, sin_own)
            q_inv[:, pair(c)] = inv
            turned = turned * score_scale
            grads = do_buf[:, pair(c)].astype(F32)
            g, r = divmod(2 * c, per_group)
            for a, (query, grad) in enumerate([(turned, shift(grads)), (shift(turned), grads)]):
                to = pl.ds((r + a) * rows, rows)
                q_st[g, to, :] = jnp.where(low_lanes, query, 0.0).astype(BF16)
                do_st[g, to, :] = jnp.where(low_lanes, 0.0, grad).astype(BF16)

    def take_kv(src, g):
        arrived(kv_all.at[src, g], kv_recv.at[src, g])

    def relay(src, g, where):
        take_kv(src, g)
        send_kv(src, g, 2 + src, where)

    def relays(turns):
        @pl.when(jnp.logical_not(is_end))
        def _():
            for src, g in turns:
                relay([other_mid, other_end][src], g, partner)

    turns = sorted(
        [(0, g) for g in range(heads)] + [(1, g) for g in range(heads)],
        key=lambda turn: turn[1] + 1.5 * turn[0],
    )
    with jax.named_scope("relay"):
        relays(turns)

    def attend(g):
        kv = kv_all[:, g].reshape(n * rows, LANES)
        both = None
        score_grads = []
        for r in range(per_group):
            at = pl.ds(r * rows, rows)
            queries = q_st[g, at, :]
            grads = do_st[g, at, :]
            scores = contract(kv, queries, ((1,), (1,)))
            prob_grad = contract(kv, grads, ((1,), (1,)))
            shifted = jnp.exp(scores - jnp.max(scores, axis=0, keepdims=True))
            prob = shifted * (1.0 / jnp.sum(shifted, axis=0, keepdims=True))
            row_dot = jnp.sum(prob * prob_grad, axis=0, keepdims=True)
            score_grad = (prob * (prob_grad - row_dot)).astype(BF16)
            term = contract(score_grad, queries, ((1,), (0,)))
            term = term + contract(prob.astype(BF16), grads, ((1,), (0,)))
            both = term if both is None else both + term
            score_grads.append(score_grad)
        part[g] = both.astype(BF16).reshape(n, rows, LANES)
        return kv, score_grads

    def query_part(g, kv, score_grads):
        parts = [contract(kv[:, :HEAD_CHANNELS], a, ((0,), (0,))) for a in score_grads]
        for r in range(0, per_group, 2):
            head = g * per_group + r
            dq_acc[:, head * HEAD_CHANNELS:head * HEAD_CHANNELS + LANES] = jnp.concatenate(
                [parts[r], parts[r + 1]], axis=0
            ).T

    def send_parts(g):
        @pl.when(is_end)
        def _():
            for i, where in enumerate([other_end, other_mid]):
                send(part.at[g, where], comb_in.at[g, i], p_send.at[0], c_recv.at[g, i],
                     {"sp": partner})

        send(part.at[g, partner], got.at[g, 0], p_send.at[0], p_recv.at[g], {"sp": partner})

    def combine(g):
        @pl.when(jnp.logical_not(is_end))
        def _():
            for i, where in enumerate([other_end, other_mid]):
                arrived(comb_in.at[g, i], c_recv.at[g, i])
                total = comb_in[g, i].astype(F32) + part[g, where].astype(F32)
                comb[g, i] = total.astype(BF16)
                send(comb.at[g, i], got.at[g, 1], p_send.at[0], p_recv.at[g], {"sp": where})

    def own_grads(g):
        with jax.named_scope(f"gotwait{g}"):
            arrived(got.at[g], p_recv.at[g])
        total = part[g, me].astype(F32) + got[g, 0].astype(F32) + got[g, 1].astype(F32)
        keys = k_head[g]
        inv = lax.rsqrt(head_mean(keys * keys) + norm_eps)
        back = norm_rotate_back(keys, inv, total, k_gain, cos_own, sin_own)
        both = jnp.where(low_lanes, back, total).astype(BF16)
        g_all[g, md] = both
        mine = g_all.at[g, md]
        for o in range(2, dp, 2):
            send(mine, mine, g_send.at[0], gd_recv.at[g], {"dp": dp_peer(o)})
        send(mine, mine, g_send.at[0], gm_recv.at[g], {"dp": mate})
        at = slice(g * HEAD_CHANNELS, (g + 1) * HEAD_CHANNELS)
        own_k[:, at] = both[:, :HEAD_CHANNELS]
        own_v[:, at] = both[:, HEAD_CHANNELS:]

    def pass_on(g):
        with jax.named_scope(f"gdwait{g}"):
            arrived(g_all.at[g, pl.ds(0, near_chips)], gd_recv.at[g])
        for o in range(2, dp, 2):
            block = g_all.at[g, dp_from(o)]
            send(block, block, g_send.at[1], gm_recv.at[g], {"dp": mate})

    def weight_grads(g):
        with jax.named_scope(f"gmwait{g}"):
            arrived(g_all.at[g, pl.ds(0, dp // 2)], gm_recv.at[g])
        total = contract(x_t[...], g_all[g].reshape(dp * rows, LANES), ((1,), (0,)))
        wg_part[g] = total.astype(BF16).reshape(2, half_share, LANES)

        def give(half, where):
            send(wg_part.at[g, half], wg_got.at[g, core * n + me], r_send.at[0],
                 r_recv.at[g, core], {"sp": where, "dp": upper})

        give(other_mid - first_mid, other_mid)

        @pl.when(jnp.logical_not(is_owner))
        def _():
            give(side_mid - first_mid, side_mid)

    def sum_weight_grads(g):
        @pl.when(is_owner)
        def _():
            mine = me - first_mid
            with jax.named_scope(f"rwait{g}"):
                arrived(wg_got.at[g, pl.ds(0, last)], r_recv.at[g, 1])
            total = wg_part[g, mine].astype(F32)
            for o in range(1, n):
                total = total + wg_got[g, n + sp_from(o)].astype(F32)
            fin_all[g, mine] = total.astype(BF16)
            with jax.named_scope(f"rwaits{g}"):
                arrived(wg_got.at[g, pl.ds(0, n)], r_recv.at[g, 0])
            total = wg_got[g, 0].astype(F32)
            for src in range(1, n):
                total = total + wg_got[g, src].astype(F32)
            fin_low[g] = total.astype(BF16)
            for block, d in ((fin_low.at[g], mate), (fin_all.at[g, mine], md)):
                for where in (other_mid, partner):
                    send(block, fin_all.at[g, mine], r_send.at[1], f_recv.at[g],
                         {"sp": where, "dp": d})
                if g >= relayed:
                    send(block, fin_all.at[g, mine], r_send.at[3], f_recv.at[g],
                         {"sp": other_end, "dp": d})
            send(fin_low.at[g], fin_all.at[g, mine], r_send.at[1], f_recv.at[g], {"dp": mate})

    def put_weight_grads(g):
        with jax.named_scope(f"fwait{g}"):
            @pl.when(is_owner)
            def _():
                arrived(fin_all.at[g, 0], f_recv.at[g])

            @pl.when(jnp.logical_not(is_owner))
            def _():
                arrived(fin_all.at[g], f_recv.at[g])
        if g < relayed:
            @pl.when(jnp.logical_not(is_end))
            def _():
                block = fin_all.at[g, other_mid - first_mid]
                send(block, block, r_send.at[2], f_recv.at[g], {"sp": partner})
        total = fin_all[g].reshape(share, LANES).astype(F32)
        at = slice(g * HEAD_CHANNELS, (g + 1) * HEAD_CHANNELS)
        kw_buf[:, at] = total[:, :HEAD_CHANNELS]
        vw_buf[:, at] = total[:, HEAD_CHANNELS:]

    def query_grads(c):
        dq_buf[:, pair(c)] = norm_rotate_back(
            q_buf[:, pair(c)].astype(F32), q_inv[:, pair(c)], dq_acc[:, pair(c)],
            q_gain * score_scale, cos_own, sin_own,
        ).astype(BF16)

    def project(src):
        out = contract(own_k[...], wk_all[src], ((1,), (1,)))
        out = out + contract(own_v[...], wv_all[src], ((1,), (1,)))
        dx_buf[:, columns(src)] = out.astype(BF16)

    blocks = q_width // LANES
    for g in range(heads):
        with jax.named_scope(f"kvwait{g}"):
            take_kv(partner, g)

            @pl.when(is_end)
            def _():
                take_kv(other_mid, g)
                take_kv(other_end, g)
        with jax.named_scope(f"attend{g}"):
            kept = attend(g)
            send_parts(g)
            query_part(g, *kept)
    with jax.named_scope("xt"):
        for copy in local[8:]:
            copy.wait()
        arrived(x_all.at[pl.ds(0, dp - 1)], x_sem.at[1])
        for src in range(dp):
            x_t[:, src * rows:(src + 1) * rows] = x_all[src].T
    def scoped(name, step, *args):
        with jax.named_scope(name):
            step(*args)

    def query_half(first):
        for c in range(first, first + blocks // 2):
            query_grads(c)

    scoped("comb0", combine, 0)
    scoped("comb1", combine, 1)
    scoped("dqa", query_half, 0)
    scoped("own0", own_grads, 0)
    scoped("comb2", combine, 2)
    scoped("comb3", combine, 3)
    scoped("own1", own_grads, 1)
    scoped("own2", own_grads, 2)
    scoped("pass0", pass_on, 0)
    scoped("own3", own_grads, 3)
    send_weights(2)
    scoped("dqb", query_half, blocks // 2)
    scoped("pass1", pass_on, 1)
    scoped("wg0", weight_grads, 0)
    scoped("pass2", pass_on, 2)
    scoped("wg1", weight_grads, 1)
    scoped("pass3", pass_on, 3)
    scoped("wg2", weight_grads, 2)
    scoped("wg3", weight_grads, 3)
    with jax.named_scope("wpass"):
        pass_weights(0)
        pass_weights(1)
    scoped("sum0", sum_weight_grads, 0)
    scoped("wlate", pass_weights, 2)
    scoped("sum1", sum_weight_grads, 1)
    with jax.named_scope("proja"):
        for o in range(0, dp, 2):
            project(dp_from(o))
    scoped("sum2", sum_weight_grads, 2)
    with jax.named_scope("wfin"):
        for kind in range(3):
            finish_weights(kind)
    with jax.named_scope("projb"):
        for o in range(0, dp, 2):
            project(mate_from(o))
    scoped("put0", put_weight_grads, 0)
    scoped("sum3", sum_weight_grads, 3)
    for g in range(1, heads):
        scoped(f"put{g}", put_weight_grads, g)

    with jax.named_scope("drain"):
        departed(kv_all.at[me], kv_send.at[0])
        departed(kv_all.at[me], kv_send.at[1])

        @pl.when(jnp.logical_not(is_end))
        def _():
            departed(kv_all.at[other_mid], kv_send.at[2 + other_mid])
            departed(kv_all.at[other_end], kv_send.at[2 + other_end])

        departed(x_all.at[pl.ds(0, dp - 1)], x_sem.at[0])
        for kind, (_, dst, at) in enumerate(weights):
            departed(dst.at[pl.ds(0, dp - 1), at], w_send.at[kind])
        departed(part.at[:, pl.ds(0, 3)], p_send.at[0])
        departed(g_all.at[:, pl.ds(0, dp // 2)], g_send.at[0])
        departed(g_all.at[:, pl.ds(0, near_chips)], g_send.at[1])

        @pl.when(is_owner)
        def _():
            departed(wg_part.at[:, 0], r_send.at[0])
            departed(wg_got.at[:, pl.ds(0, 5)], r_send.at[1])
            departed(wg_got.at[pl.ds(0, heads - relayed), pl.ds(0, 2)], r_send.at[3])

        @pl.when(jnp.logical_not(is_owner))
        def _():
            departed(wg_part, r_send.at[0])

        @pl.when(jnp.logical_not(is_end))
        def _():
            departed(fin_low.at[pl.ds(0, relayed)], r_send.at[2])


def write_kernel(*refs):
    count = (len(refs) - 1) // 2
    copies = [
        pltpu.make_async_copy(refs[i], refs[count + i], refs[-1].at[i]) for i in range(count)
    ]
    for copy in copies:
        copy.start()
    for copy in copies:
        copy.wait()


def kernel_step(
    n, dp, inputs, queries, keys, values, out_grad, query_gain, key_gain, key_matrix, value_matrix
):
    rows, width = inputs.shape[1:]
    q_width = queries.shape[2]
    kv_width = keys.shape[2]
    length = rows * n
    share = width // dp
    kv_heads = kv_width // HEAD_CHANNELS
    stack = rows * (q_width // kv_width)
    cos_tab, sin_tab = pair_tables(length)
    vmem = pltpu.VMEM
    dma = pltpu.SemaphoreType.DMA
    packed = (rows, LANES)
    scratch = [
        vmem((1, HEAD_CHANNELS), F32), vmem((1, HEAD_CHANNELS), F32),
        vmem((rows, q_width), BF16), vmem((rows, q_width), BF16),
        vmem(packed, F32), vmem(packed, F32),
        vmem((rows, kv_width), BF16), vmem((rows, kv_width), BF16),
        vmem((kv_heads, *packed), F32), vmem((n, kv_heads, *packed), BF16),
        vmem((rows, q_width), F32),
        vmem((kv_heads, stack, LANES), BF16), vmem((kv_heads, stack, LANES), BF16),
        vmem((dp, rows, share), BF16), vmem((share, dp * rows), BF16),
        vmem((dp, share, kv_width), BF16), vmem((dp, share, kv_width), BF16),
        vmem((rows, q_width), F32),
        vmem((kv_heads, n, *packed), BF16),
        vmem((kv_heads, 2, *packed), BF16), vmem((kv_heads, 2, *packed), BF16),
        vmem((kv_heads, 2, *packed), BF16),
        vmem((kv_heads, dp, *packed), BF16),
        vmem((rows, kv_width), BF16), vmem((rows, kv_width), BF16),
        vmem((kv_heads, 2, share // 2, LANES), BF16),
        vmem((kv_heads, 2 * n, share // 2, LANES), BF16),
        vmem((kv_heads, 2, share // 2, LANES), BF16), vmem((kv_heads, share // 2, LANES), BF16),
        dma((11,)), dma((2 + n,)), dma((n, kv_heads)), dma((2,)), dma((3,)), dma((3, 2)),
        dma((1,)), dma((kv_heads, 2)), dma((kv_heads,)),
        dma((2,)), dma((kv_heads,)), dma((kv_heads,)),
        dma((4,)), dma((kv_heads, 2)), dma((kv_heads,)),
    ]
    hbm = pl.BlockSpec(memory_space=pltpu.HBM)
    here = pl.BlockSpec(memory_space=pltpu.VMEM)
    results = [
        ((rows, width), BF16), ((rows, q_width), BF16),
        ((share, kv_width), F32), ((share, kv_width), F32),
    ]
    held_bytes = 65536 + sum(a * b * jnp.dtype(kind).itemsize for (a, b), kind in results)
    held = pl.pallas_call(
        functools.partial(step_kernel, n, dp),
        out_shape=[pltpu.VMEM(shape, kind) for shape, kind in results],
        in_specs=[hbm] * 11,
        out_specs=[here] * 4,
        scratch_shapes=scratch,
        compiler_params=pltpu.CompilerParams(
            collective_id=0, has_side_effects=True, vmem_limit_bytes=VMEM_BYTES - held_bytes
        ),
    )(
        inputs[0], queries[0], keys[0], values[0], out_grad[0],
        query_gain[None], key_gain[None],
        key_matrix, value_matrix, jnp.asarray(cos_tab), jnp.asarray(sin_tab),
    )
    dx, dq, kw, vw = pl.pallas_call(
        write_kernel,
        out_shape=[jax.ShapeDtypeStruct(shape, kind) for shape, kind in results],
        in_specs=[here] * 4,
        out_specs=[hbm] * 4,
        scratch_shapes=[dma((4,))],
        compiler_params=pltpu.CompilerParams(vmem_limit_bytes=8 * 1024 * 1024),
    )(*held)
    return dx[None], dq[None], kw, vw


def device_step(inputs, *rest):
    n = lax.axis_size("sp")
    dp = lax.axis_size("dp")
    rows, width = inputs.shape[1:]
    fits = n == 4 and dp == 8 and width % (dp * LANES) == 0 and rows == LANES
    if fits and (width // dp) % (32 * n) == 0:
        return kernel_step(n, dp, inputs, *rest)
    return on_device(inputs, *rest)


def solution(mesh):
    return jax.shard_map(
        device_step,
        mesh=mesh,
        in_specs=(
            P("dp", "sp", None),
            P("dp", "sp", None),
            P("dp", "sp", None),
            P("dp", "sp", None),
            P("dp", "sp", None),
            P(),
            P(),
            P("dp", None),
            P("dp", None),
        ),
        out_specs=(P("dp", "sp", None), P("dp", "sp", None), P("dp", None), P("dp", None)),
        check_vma=False,
    )
```

```python
import functools

import jax
import jax.numpy as jnp
import numpy as np
from jax import lax
from jax.experimental import pallas as pl
from jax.experimental.pallas import tpu as pltpu
from jax.sharding import PartitionSpec as P

QUERY_HEADS = 16
KEY_VALUE_HEADS = 4
HEAD_CHANNELS = 64
GRID = 64


rope_base = 10000.0
norm_eps = 0.5
score_scale = 0.125


def product(pattern, first_op, second_op):
    return jnp.einsum(pattern, first_op, second_op, preferred_element_type=jnp.float32)


def rotary_tables(token_length):
    position = jnp.arange(token_length, dtype=jnp.int32)
    grid_row = (position // GRID).astype(jnp.float32)
    grid_col = (position % GRID).astype(jnp.float32)
    half_pairs = HEAD_CHANNELS // 4
    inv_freq = rope_base ** (-jnp.arange(half_pairs, dtype=jnp.float32) / half_pairs)
    angles = jnp.concatenate([grid_row[:, None] * inv_freq, grid_col[:, None] * inv_freq], axis=1)
    return (jnp.cos(angles), jnp.sin(angles))


def rotate(vector, cos_tab, sin_tab):
    even_part = vector[..., 0::2]
    odd_part = vector[..., 1::2]
    turned = jnp.stack(
        [even_part * cos_tab - odd_part * sin_tab, even_part * sin_tab + odd_part * cos_tab],
        axis=-1,
    )
    return turned.reshape(vector.shape)


def rotate_back(cotangent, cos_tab, sin_tab):
    even_part = cotangent[..., 0::2]
    odd_part = cotangent[..., 1::2]
    turned = jnp.stack(
        [even_part * cos_tab + odd_part * sin_tab, odd_part * cos_tab - even_part * sin_tab],
        axis=-1,
    )
    return turned.reshape(cotangent.shape)


def inverse_rms(vector):
    return lax.rsqrt(jnp.mean(vector * vector, axis=-1, keepdims=True) + norm_eps)


def norm_back(vector, inv_scale, cotangent, gain_vec):
    weighted = cotangent * gain_vec
    inner_mean = jnp.mean(weighted * vector, axis=-1, keepdims=True)
    return inv_scale * (weighted - vector * inv_scale * inv_scale * inner_mean)


def head_grads(
    query_in, key_input, value_input, grad_in, query_gain, key_gain, cos_tab, sin_tab, block_rows
):
    token_length, groups, per_group, head_dim = query_in.shape
    cos_four = cos_tab[:, None, None, :]
    sin_four = sin_tab[:, None, None, :]
    cos_three = cos_tab[:, None, :]
    sin_three = sin_tab[:, None, :]
    query_f = query_in.astype(jnp.float32)
    query_inv = inverse_rms(query_f)
    query_rot = rotate(query_f * query_inv * query_gain, cos_four, sin_four).astype(jnp.bfloat16)
    key_f = key_input.astype(jnp.float32)
    key_inv = inverse_rms(key_f)
    key_rot = rotate(key_f * key_inv * key_gain, cos_three, sin_three).astype(jnp.bfloat16)
    num_blocks = token_length // block_rows
    query_blocks = query_rot.reshape(num_blocks, block_rows, groups, per_group, head_dim)
    grad_blocks = grad_in.reshape(num_blocks, block_rows, groups, per_group, head_dim)

    def attend_block(carried, pieces):
        key_acc, value_acc = carried
        query_piece, grad_piece = pieces
        scores = product("qgrd,cgd->grqc", query_piece, key_rot) * score_scale
        row_max = jnp.max(scores, axis=-1, keepdims=True)
        shifted = jnp.exp(scores - row_max)
        attn_prob = shifted / jnp.sum(shifted, axis=-1, keepdims=True)
        prob_low = attn_prob.astype(jnp.bfloat16)
        prob_grad = product("qgrd,cgd->grqc", grad_piece, value_input)
        row_dot = jnp.sum(attn_prob * prob_grad, axis=-1, keepdims=True)
        score_grad = (attn_prob * (prob_grad - row_dot) * score_scale).astype(jnp.bfloat16)
        dq_piece = product("grqc,cgd->qgrd", score_grad, key_rot)
        key_acc = key_acc + product("grqc,qgrd->cgd", score_grad, query_piece)
        value_acc = value_acc + product("grqc,qgrd->cgd", prob_low, grad_piece)
        return ((key_acc, value_acc), dq_piece)

    empty_acc = jnp.zeros((token_length, groups, head_dim), jnp.float32)
    (key_rot_grad, value_acc), query_rot_grad = lax.scan(
        attend_block, (empty_acc, empty_acc), (query_blocks, grad_blocks)
    )
    query_rot_grad = query_rot_grad.reshape(token_length, groups, per_group, head_dim)
    query_grad = norm_back(
        query_f, query_inv, rotate_back(query_rot_grad, cos_four, sin_four), query_gain
    ).astype(jnp.bfloat16)
    key_portion = norm_back(
        key_f, key_inv, rotate_back(key_rot_grad, cos_three, sin_three), key_gain
    ).astype(jnp.bfloat16)
    return (query_grad, key_portion, value_acc.astype(jnp.bfloat16))


def on_device(
    inputs, queries, keys, values, out_grad, query_gain, key_gain, key_matrix, value_matrix
):
    sp_count = lax.axis_size("sp")
    dp_count = lax.axis_size("dp")
    token_row_block = inputs.shape[1]
    token_length = token_row_block * sp_count
    local_heads = QUERY_HEADS // sp_count
    portion_heads = min(local_heads, QUERY_HEADS // KEY_VALUE_HEADS)
    kv_here = local_heads // portion_heads
    group_copies = QUERY_HEADS // KEY_VALUE_HEADS // portion_heads
    key_value_width = KEY_VALUE_HEADS * HEAD_CHANNELS
    key_positions = jnp.repeat(
        keys[0].reshape(token_row_block, KEY_VALUE_HEADS, HEAD_CHANNELS), group_copies, axis=1
    ).reshape(token_row_block, key_value_width * group_copies)
    value_positions = jnp.repeat(
        values[0].reshape(token_row_block, KEY_VALUE_HEADS, HEAD_CHANNELS), group_copies, axis=1
    ).reshape(token_row_block, key_value_width * group_copies)
    grad_heads, query_heads, key_heads, value_heads = (
        lax.all_to_all(out_grad[0], "sp", split_axis=1, concat_axis=0, tiled=True),
        lax.all_to_all(queries[0], "sp", split_axis=1, concat_axis=0, tiled=True),
        lax.all_to_all(key_positions, "sp", split_axis=1, concat_axis=0, tiled=True),
        lax.all_to_all(value_positions, "sp", split_axis=1, concat_axis=0, tiled=True),
    )
    cos_tab, sin_tab = rotary_tables(token_length)
    query_part, key_portion, value_portion = head_grads(
        query_heads.reshape(token_length, kv_here, portion_heads, HEAD_CHANNELS),
        key_heads.reshape(token_length, kv_here, HEAD_CHANNELS),
        value_heads.reshape(token_length, kv_here, HEAD_CHANNELS),
        grad_heads.reshape(token_length, kv_here, portion_heads, HEAD_CHANNELS),
        query_gain,
        key_gain,
        cos_tab,
        sin_tab,
        min(512, token_length),
    )
    query_tokens, key_token_rows, value_token_rows = (
        lax.all_to_all(
            query_part.reshape(token_length, local_heads * HEAD_CHANNELS),
            "sp",
            split_axis=0,
            concat_axis=1,
            tiled=True,
        ),
        lax.all_to_all(
            key_portion.reshape(token_length, kv_here * HEAD_CHANNELS),
            "sp",
            split_axis=0,
            concat_axis=1,
            tiled=True,
        ),
        lax.all_to_all(
            value_portion.reshape(token_length, kv_here * HEAD_CHANNELS),
            "sp",
            split_axis=0,
            concat_axis=1,
            tiled=True,
        ),
    )
    key_gradient = (
        key_token_rows.reshape(token_row_block, KEY_VALUE_HEADS, group_copies, HEAD_CHANNELS)
        .astype(jnp.float32)
        .sum(axis=2)
        .astype(jnp.bfloat16)
    )
    value_gradient = (
        value_token_rows.reshape(token_row_block, KEY_VALUE_HEADS, group_copies, HEAD_CHANNELS)
        .astype(jnp.float32)
        .sum(axis=2)
        .astype(jnp.bfloat16)
    )
    projection_gradient = jnp.concatenate(
        [
            key_gradient.reshape(token_row_block, key_value_width),
            value_gradient.reshape(token_row_block, key_value_width),
        ],
        axis=1,
    )
    joined_weight = jnp.concatenate([key_matrix, value_matrix], axis=1)
    input_grad = lax.dot_general(
        projection_gradient,
        lax.all_gather(joined_weight, "dp", axis=0, tiled=True),
        (((1,), (1,)), ((), ())),
        preferred_element_type=jnp.float32,
    ).astype(jnp.bfloat16)
    token_in = inputs[0]
    width = inputs.shape[2]
    row_share = width // (sp_count * dp_count)
    permuted = (
        token_in.reshape(token_row_block, dp_count, sp_count, row_share)
        .transpose(0, 2, 1, 3)
        .reshape(token_row_block, width)
    )
    share_cols = lax.all_to_all(permuted, "sp", split_axis=1, concat_axis=0, tiled=True)
    all_grads = lax.all_gather(projection_gradient, "sp", axis=0, tiled=True)
    grad_piece = lax.psum_scatter(
        lax.dot_general(
            share_cols, all_grads, (((0,), (0,)), ((), ())), preferred_element_type=jnp.float32
        ).astype(jnp.bfloat16),
        "dp",
        scatter_dimension=0,
        tiled=True,
    ).astype(jnp.float32)
    weight_grad = lax.all_gather(grad_piece, "sp", axis=0, tiled=True)
    return (
        input_grad[None],
        query_tokens[None],
        weight_grad[:, :key_value_width],
        weight_grad[:, key_value_width:],
    )


LANES = 128
VMEM_BYTES = 67043328
MESH = pl.DeviceIdType.MESH
F32 = jnp.float32
BF16 = jnp.bfloat16


def pair_tables(token_length):
    position = np.arange(token_length)
    half_pairs = HEAD_CHANNELS // 4
    inv_freq = (rope_base ** (-np.arange(half_pairs) / half_pairs)).astype(np.float32)
    row = (position // GRID).astype(np.float32)
    col = (position % GRID).astype(np.float32)
    angles = np.concatenate([row[:, None] * inv_freq, col[:, None] * inv_freq], axis=1)
    cos_tab = np.repeat(np.cos(angles), 2, axis=1)
    sin_tab = np.repeat(np.sin(angles), 2, axis=1)
    sin_tab[:, 0::2] *= -1.0
    return (
        np.tile(cos_tab, (1, 2)).astype(np.float32),
        np.tile(sin_tab, (1, 2)).astype(np.float32),
    )


def swap_pairs(x):
    lane = lax.broadcasted_iota(jnp.int32, x.shape, 1)
    return jnp.where(lane % 2 == 0, pltpu.roll(x, LANES - 1, 1), pltpu.roll(x, 1, 1))


def head_mean(z):
    row = lax.broadcasted_iota(jnp.int32, (LANES, LANES), 0) // HEAD_CHANNELS
    col = lax.broadcasted_iota(jnp.int32, (LANES, LANES), 1) // HEAD_CHANNELS
    ones = jnp.where(row == col, 1.0, 0.0).astype(BF16)
    high = z.astype(BF16)
    low = (z - high.astype(F32)).astype(BF16)
    total = jnp.dot(high, ones, preferred_element_type=F32)
    total = total + jnp.dot(low, ones, preferred_element_type=F32)
    return total * (1.0 / HEAD_CHANNELS)


def norm_rotate(x, gain, cos_tab, sin_tab):
    inv = lax.rsqrt(head_mean(x * x) + norm_eps)
    y = x * inv * gain
    return y * cos_tab + swap_pairs(y) * sin_tab, inv


def norm_rotate_back(x, inv, cotangent, gain, cos_tab, sin_tab):
    turned = cotangent * cos_tab - swap_pairs(cotangent) * sin_tab
    weighted = turned * gain
    return inv * (weighted - x * (inv * inv * head_mean(weighted * x)))


def contract(a, b, dims):
    return lax.dot_general(a, b, (dims, ((), ())), preferred_element_type=F32)


def step_kernel(
    n, dp,
    x_hbm, q_hbm, k_hbm, v_hbm, do_hbm, qg_hbm, kg_hbm, km_hbm, vm_hbm, cos_hbm, sin_hbm,
    dx_buf, dq_buf, kw_buf, vw_buf,
    qg_ref, kg_ref, q_buf, do_buf, cos_buf, sin_buf, k_own, v_own, k_head, kv_all, q_inv, q_st, do_st,
    x_all, x_t, wk_all, wv_all, dq_acc, part, comb_in, comb, got, g_all, own_k, own_v,
    wg_part, wg_got, fin_all, fin_low,
    local_sem, kv_send, kv_recv, x_sem, w_send, w_recv, p_send, c_recv, p_recv,
    g_send, gd_recv, gm_recv, r_send, r_recv, f_recv,
):
    me = lax.axis_index("sp")
    md = lax.axis_index("dp")
    rows, q_width = q_buf.shape
    heads = kv_all.shape[1]
    share = x_all.shape[2]
    per_group = q_width // (heads * HEAD_CHANNELS)
    half_share = share // 2
    mate = md + 1 - 2 * (md % 2)
    last = n - 1
    first_mid = n // 2 - 1
    partner = me + 1 - 2 * (me % 2)
    low_side = me < n // 2
    other_end = jnp.where(low_side, last, 0)
    other_mid = jnp.where(low_side, n // 2, n // 2 - 1)
    is_end = jnp.logical_or(me == 0, me == last)
    near_chips = dp // 2 - 1
    core = md % 2
    upper = md + 1 - core
    side_mid = jnp.where(is_end, partner, me)
    is_owner = jnp.logical_and(jnp.logical_not(is_end), core == 1)
    first_straight = 0
    relayed = 1

    def sp_peer(o):
        return lax.rem(me + o, n)

    def sp_from(o):
        return lax.rem(me - o + n, n)

    def dp_peer(o):
        return lax.rem(md + o, dp)

    def dp_from(o):
        return lax.rem(md - o + dp, dp)

    def mate_from(o):
        return lax.rem(mate - o + dp, dp)

    def pair(c):
        return pl.ds(c * LANES, LANES)

    def columns(d):
        return pl.ds(pl.multiple_of(d * share, share), share)

    barrier = pltpu.get_barrier_semaphore()

    def greet(where):
        pl.semaphore_signal(barrier, inc=1, device_id=where, device_id_type=MESH)

    @pl.when(me > 0)
    def _():
        greet({"sp": me - 1})

    @pl.when(me < last)
    def _():
        greet({"sp": me + 1})

    @pl.when(jnp.logical_not(is_end))
    def _():
        greet({"sp": other_end})

    for o in range(1, dp):
        greet({"dp": dp_peer(o)})

    my_rows = pl.ds(pl.multiple_of(me * rows, rows), rows)
    wanted = [
        (k_hbm, k_own), (v_hbm, v_own), (cos_hbm.at[my_rows, :], cos_buf),
        (sin_hbm.at[my_rows, :], sin_buf), (kg_hbm, kg_ref), (qg_hbm, qg_ref),
        (q_hbm, q_buf), (do_hbm, do_buf),
        (x_hbm.at[:, columns(md)], x_all.at[md]), (km_hbm, wk_all.at[md]), (vm_hbm, wv_all.at[md]),
    ]
    local = [
        pltpu.make_async_copy(src, dst, local_sem.at[i]) for i, (src, dst) in enumerate(wanted)
    ]
    for copy in local:
        copy.start()

    def remote(src, dst, send, recv, where):
        return pltpu.make_async_remote_copy(
            src_ref=src, dst_ref=dst, send_sem=send, recv_sem=recv,
            device_id=where, device_id_type=MESH,
        )

    def send(*args):
        remote(*args).start()

    def arrived(dst, recv):
        remote(dst, dst, recv, recv, {"sp": me}).wait_recv()

    def departed(src, sem):
        remote(src, src, sem, sem, {"sp": me}).wait_send()

    low_lanes = lax.broadcasted_iota(jnp.int32, (rows, LANES), 1) < HEAD_CHANNELS

    def shift(a):
        return pltpu.roll(a, HEAD_CHANNELS, 1)

    with jax.named_scope("local"):
        for copy in local[:6]:
            copy.wait()
    cos_own = cos_buf[...]
    sin_own = sin_buf[...]
    q_gain = jnp.concatenate([qg_ref[...], qg_ref[...]], axis=1)
    k_gain = jnp.concatenate([kg_ref[...], kg_ref[...]], axis=1)

    for c in range(heads // 2):
        keys = k_own[:, pair(c)].astype(F32)
        vals = v_own[:, pair(c)].astype(F32)
        turned = norm_rotate(keys, k_gain, cos_own, sin_own)[0]
        kv_all[me, 2 * c] = jnp.where(low_lanes, turned, shift(vals)).astype(BF16)
        kv_all[me, 2 * c + 1] = jnp.where(low_lanes, shift(turned), vals).astype(BF16)
        k_head[2 * c] = keys
        k_head[2 * c + 1] = shift(keys)

    with jax.named_scope("barrier"):
        pl.semaphore_wait(barrier, dp + 1)

    def send_kv(src, g, sem, where):
        block = kv_all.at[src, g]
        send(block, block, kv_send.at[sem], kv_recv.at[src, g], {"sp": where})

    for g in range(heads):
        send_kv(me, g, 0, other_mid)
        send_kv(me, g, 1, partner)

    for o in range(1, dp):
        send(x_hbm.at[:, columns(dp_peer(o))], x_all.at[md], x_sem.at[0], x_sem.at[1],
             {"dp": dp_peer(o)})

    top = pl.ds(0, half_share)
    bottom = pl.ds(half_share, half_share)
    full = pl.ds(0, share)
    weights = [(km_hbm, wk_all, full), (vm_hbm, wv_all, top), (vm_hbm, wv_all, bottom)]

    def send_weights(kind):
        src, dst, at = weights[kind]
        for o in range(2, dp, 2):
            send(src.at[at], dst.at[md, at], w_send.at[kind], w_recv.at[kind, 0],
                 {"dp": dp_peer(o)})
        send(src.at[at], dst.at[md, at], w_send.at[kind], w_recv.at[kind, 1], {"dp": mate})

    def pass_weights(kind):
        _, dst, at = weights[kind]
        arrived(dst.at[pl.ds(0, near_chips), at], w_recv.at[kind, 0])
        for o in range(2, dp, 2):
            block = dst.at[dp_from(o), at]
            send(block, block, w_send.at[kind], w_recv.at[kind, 1], {"dp": mate})

    def finish_weights(kind):
        _, dst, at = weights[kind]
        arrived(dst.at[pl.ds(0, dp // 2), at], w_recv.at[kind, 1])

    send_weights(0)
    send_weights(1)

    with jax.named_scope("local2"):
        for copy in local[6:8]:
            copy.wait()
    with jax.named_scope("qrot"):
        for c in range(q_width // LANES):
            turned, inv = norm_rotate(q_buf[:, pair(c)].astype(F32), q_gain, cos_own, sin_own)
            q_inv[:, pair(c)] = inv
            turned = turned * score_scale
            grads = do_buf[:, pair(c)].astype(F32)
            g, r = divmod(2 * c, per_group)
            for a, (query, grad) in enumerate([(turned, shift(grads)), (shift(turned), grads)]):
                to = pl.ds((r + a) * rows, rows)
                q_st[g, to, :] = jnp.where(low_lanes, query, 0.0).astype(BF16)
                do_st[g, to, :] = jnp.where(low_lanes, 0.0, grad).astype(BF16)

    def take_kv(src, g):
        arrived(kv_all.at[src, g], kv_recv.at[src, g])

    def relay(src, g, where):
        take_kv(src, g)
        send_kv(src, g, 2 + src, where)

    def relays(turns):
        @pl.when(jnp.logical_not(is_end))
        def _():
            for src, g in turns:
                relay([other_mid, other_end][src], g, partner)

    turns = sorted(
        [(0, g) for g in range(heads)] + [(1, g) for g in range(heads)],
        key=lambda turn: turn[1] + 0.5 * turn[0],
    )
    with jax.named_scope("relay"):
        relays(turns)

    step = 1

    def attend(g):
        kv = kv_all[:, g].reshape(n * rows, LANES)
        both = None
        score_grads = []
        for r in range(0, per_group, step):
            at = pl.ds(r * rows, step * rows)
            queries = q_st[g, at, :]
            grads = do_st[g, at, :]
            scores = contract(kv, queries, ((1,), (1,)))
            prob_grad = contract(kv, grads, ((1,), (1,)))
            shifted = jnp.exp(scores - jnp.max(scores, axis=0, keepdims=True))
            inverse = 1.0 / jnp.sum(shifted, axis=0, keepdims=True)
            prob = shifted * inverse
            row_dot = jnp.sum(prob * prob_grad, axis=0, keepdims=True)
            score_grad = (prob * (prob_grad - row_dot)).astype(BF16)
            term = contract(score_grad, queries, ((1,), (0,)))
            term = term + contract(prob.astype(BF16), grads, ((1,), (0,)))
            both = term if both is None else both + term
            score_grads.append(score_grad)
        part[g] = both.astype(BF16).reshape(n, rows, LANES)
        return kv, score_grads

    def query_part(g, kv, score_grads):
        parts = [contract(kv[:, :HEAD_CHANNELS], a, ((0,), (0,))) for a in score_grads]
        for r in range(0, per_group, 2):
            head = g * per_group + r
            dq_acc[:, head * HEAD_CHANNELS:head * HEAD_CHANNELS + LANES] = jnp.concatenate(
                [parts[r], parts[r + 1]], axis=0
            ).T

    def straight(g):
        return core == 0 if g >= first_straight else core < 0

    def send_parts(g):
        @pl.when(straight(g))
        def _():
            for where in (other_end, other_mid):
                send(part.at[g, where], got.at[g, jnp.where(is_end, 1, 2)], p_send.at[0],
                     p_recv.at[g], {"sp": where})

        @pl.when(jnp.logical_and(is_end, jnp.logical_not(straight(g))))
        def _():
            for i, where in enumerate([other_end, other_mid]):
                send(part.at[g, where], comb_in.at[g, i], p_send.at[0], c_recv.at[g, i],
                     {"sp": partner})

        send(part.at[g, partner], got.at[g, 0], p_send.at[0], p_recv.at[g], {"sp": partner})

    def combine(g):
        @pl.when(jnp.logical_not(jnp.logical_or(is_end, straight(g))))
        def _():
            for i, where in enumerate([other_end, other_mid]):
                arrived(comb_in.at[g, i], c_recv.at[g, i])
                total = comb_in[g, i].astype(F32) + part[g, where].astype(F32)
                comb[g, i] = total.astype(BF16)
                send(comb.at[g, i], got.at[g, 1], p_send.at[0], p_recv.at[g], {"sp": where})

    def own_grads(g):
        with jax.named_scope(f"gotwait{g}"):
            @pl.when(straight(g))
            def _():
                arrived(got.at[g], p_recv.at[g])

            @pl.when(jnp.logical_not(straight(g)))
            def _():
                arrived(got.at[g, pl.ds(0, 2)], p_recv.at[g])
        total = part[g, me].astype(F32) + got[g, 0].astype(F32) + got[g, 1].astype(F32)
        total = total + jnp.where(straight(g), got[g, 2].astype(F32), 0.0)
        keys = k_head[g]
        inv = lax.rsqrt(head_mean(keys * keys) + norm_eps)
        back = norm_rotate_back(keys, inv, total, k_gain, cos_own, sin_own)
        both = jnp.where(low_lanes, back, total).astype(BF16)
        g_all[g, md] = both
        mine = g_all.at[g, md]
        for o in range(2, dp, 2):
            send(mine, mine, g_send.at[0], gd_recv.at[g], {"dp": dp_peer(o)})
        send(mine, mine, g_send.at[0], gm_recv.at[g], {"dp": mate})
        at = slice(g * HEAD_CHANNELS, (g + 1) * HEAD_CHANNELS)
        own_k[:, at] = both[:, :HEAD_CHANNELS]
        own_v[:, at] = both[:, HEAD_CHANNELS:]

    def pass_on(g):
        with jax.named_scope(f"gdwait{g}"):
            arrived(g_all.at[g, pl.ds(0, near_chips)], gd_recv.at[g])
        for o in range(2, dp, 2):
            block = g_all.at[g, dp_from(o)]
            send(block, block, g_send.at[1], gm_recv.at[g], {"dp": mate})

    def weight_grads(g):
        with jax.named_scope(f"gmwait{g}"):
            arrived(g_all.at[g, pl.ds(0, dp // 2)], gm_recv.at[g])
        total = contract(x_t[...], g_all[g].reshape(dp * rows, LANES), ((1,), (0,)))
        wg_part[g] = total.astype(BF16).reshape(2, half_share, LANES)

        def give(half, where):
            send(wg_part.at[g, half], wg_got.at[g, core * n + me], r_send.at[0],
                 r_recv.at[g, core], {"sp": where, "dp": upper})

        give(other_mid - first_mid, other_mid)

        @pl.when(jnp.logical_not(is_owner))
        def _():
            give(side_mid - first_mid, side_mid)

    def sum_weight_grads(g):
        @pl.when(is_owner)
        def _():
            mine = me - first_mid
            with jax.named_scope(f"rwait{g}"):
                arrived(wg_got.at[g, pl.ds(0, last)], r_recv.at[g, 1])
            total = wg_part[g, mine].astype(F32)
            for o in range(1, n):
                total = total + wg_got[g, n + sp_from(o)].astype(F32)
            fin_all[g, mine] = total.astype(BF16)
            with jax.named_scope(f"rwaits{g}"):
                arrived(wg_got.at[g, pl.ds(0, n)], r_recv.at[g, 0])
            total = wg_got[g, 0].astype(F32)
            for src in range(1, n):
                total = total + wg_got[g, src].astype(F32)
            fin_low[g] = total.astype(BF16)
            for block, d in ((fin_low.at[g], mate), (fin_all.at[g, mine], md)):
                for where in (other_mid, partner):
                    send(block, fin_all.at[g, mine], r_send.at[1], f_recv.at[g],
                         {"sp": where, "dp": d})
                if g >= relayed:
                    send(block, fin_all.at[g, mine], r_send.at[3], f_recv.at[g],
                         {"sp": other_end, "dp": d})
            send(fin_low.at[g], fin_all.at[g, mine], r_send.at[1], f_recv.at[g], {"dp": mate})

    def put_weight_grads(g):
        with jax.named_scope(f"fwait{g}"):
            @pl.when(is_owner)
            def _():
                arrived(fin_all.at[g, 0], f_recv.at[g])

            @pl.when(jnp.logical_not(is_owner))
            def _():
                arrived(fin_all.at[g], f_recv.at[g])
        if g < relayed:
            @pl.when(jnp.logical_not(is_end))
            def _():
                block = fin_all.at[g, other_mid - first_mid]
                send(block, block, r_send.at[2], f_recv.at[g], {"sp": partner})
        total = fin_all[g].reshape(share, LANES).astype(F32)
        at = slice(g * HEAD_CHANNELS, (g + 1) * HEAD_CHANNELS)
        kw_buf[:, at] = total[:, :HEAD_CHANNELS]
        vw_buf[:, at] = total[:, HEAD_CHANNELS:]

    def query_grads(c):
        dq_buf[:, pair(c)] = norm_rotate_back(
            q_buf[:, pair(c)].astype(F32), q_inv[:, pair(c)], dq_acc[:, pair(c)],
            q_gain * score_scale, cos_own, sin_own,
        ).astype(BF16)

    def project(src):
        out = contract(own_k[...], wk_all[src], ((1,), (1,)))
        out = out + contract(own_v[...], wv_all[src], ((1,), (1,)))
        dx_buf[:, columns(src)] = out.astype(BF16)

    blocks = q_width // LANES
    for g in range(heads):
        with jax.named_scope(f"kvwait{g}"):
            take_kv(partner, g)

            @pl.when(is_end)
            def _():
                take_kv(other_mid, g)
                take_kv(other_end, g)
        if g == heads - 1:
            with jax.named_scope("comb0"):
                combine(0)
        with jax.named_scope(f"attend{g}"):
            kept = attend(g)
            send_parts(g)
            query_part(g, *kept)
    with jax.named_scope("xt"):
        for copy in local[8:]:
            copy.wait()
        arrived(x_all.at[pl.ds(0, dp - 1)], x_sem.at[1])
        for src in range(dp):
            x_t[:, src * rows:(src + 1) * rows] = x_all[src].T
    def scoped(name, step, *args):
        with jax.named_scope(name):
            step(*args)

    def query_half(first):
        for c in range(first, first + blocks // 2):
            query_grads(c)

    scoped("comb1", combine, 1)
    scoped("dqa", query_half, 0)
    scoped("own0", own_grads, 0)
    scoped("comb2", combine, 2)
    scoped("comb3", combine, 3)
    scoped("own1", own_grads, 1)
    scoped("dqa", query_half, 0)
    scoped("own2", own_grads, 2)
    scoped("pass0", pass_on, 0)
    scoped("own3", own_grads, 3)
    send_weights(2)
    scoped("dqb", query_half, blocks // 2)
    with jax.named_scope("wpass"):
        pass_weights(0)
        pass_weights(1)
    scoped("wg0", weight_grads, 0)
    scoped("pass1", pass_on, 1)
    scoped("wg1", weight_grads, 1)
    scoped("pass2", pass_on, 2)
    scoped("pass3", pass_on, 3)
    scoped("sum0", sum_weight_grads, 0)
    scoped("wg2", weight_grads, 2)
    scoped("wg3", weight_grads, 3)
    scoped("sum1", sum_weight_grads, 1)
    scoped("wlate", pass_weights, 2)
    with jax.named_scope("proja"):
        for o in range(0, dp, 2):
            project(dp_from(o))
    scoped("sum2", sum_weight_grads, 2)
    scoped("sum3", sum_weight_grads, 3)
    with jax.named_scope("wfin"):
        for kind in range(3):
            finish_weights(kind)
    with jax.named_scope("projb"):
        for o in range(0, dp, 2):
            project(mate_from(o))
    for g in range(heads):
        scoped(f"put{g}", put_weight_grads, g)

    with jax.named_scope("drain"):
        departed(kv_all.at[me], kv_send.at[0])
        departed(kv_all.at[me], kv_send.at[1])

        @pl.when(jnp.logical_not(is_end))
        def _():
            departed(kv_all.at[other_mid], kv_send.at[2 + other_mid])
            departed(kv_all.at[other_end], kv_send.at[2 + other_end])

        departed(x_all.at[pl.ds(0, dp - 1)], x_sem.at[0])
        for kind, (_, dst, at) in enumerate(weights):
            departed(dst.at[pl.ds(0, dp - 1), at], w_send.at[kind])
        departed(part.at[:, pl.ds(0, 3)], p_send.at[0])
        departed(g_all.at[:, pl.ds(0, dp // 2)], g_send.at[0])
        departed(g_all.at[:, pl.ds(0, near_chips)], g_send.at[1])

        @pl.when(is_owner)
        def _():
            departed(wg_part.at[:, 0], r_send.at[0])
            departed(wg_got.at[:, pl.ds(0, 5)], r_send.at[1])
            departed(wg_got.at[pl.ds(0, heads - relayed), pl.ds(0, 2)], r_send.at[3])

        @pl.when(jnp.logical_not(is_owner))
        def _():
            departed(wg_part, r_send.at[0])

        @pl.when(jnp.logical_not(is_end))
        def _():
            departed(fin_low.at[pl.ds(0, relayed)], r_send.at[2])


def write_kernel(*refs):
    count = (len(refs) - 1) // 2
    copies = [
        pltpu.make_async_copy(refs[i], refs[count + i], refs[-1].at[i]) for i in range(count)
    ]
    for copy in copies:
        copy.start()
    for copy in copies:
        copy.wait()


def kernel_step(
    n, dp, inputs, queries, keys, values, out_grad, query_gain, key_gain, key_matrix, value_matrix
):
    rows, width = inputs.shape[1:]
    q_width = queries.shape[2]
    kv_width = keys.shape[2]
    length = rows * n
    share = width // dp
    kv_heads = kv_width // HEAD_CHANNELS
    stack = rows * (q_width // kv_width)
    cos_tab, sin_tab = pair_tables(length)
    vmem = pltpu.VMEM
    dma = pltpu.SemaphoreType.DMA
    packed = (rows, LANES)
    scratch = [
        vmem((1, HEAD_CHANNELS), F32), vmem((1, HEAD_CHANNELS), F32),
        vmem((rows, q_width), BF16), vmem((rows, q_width), BF16),
        vmem(packed, F32), vmem(packed, F32),
        vmem((rows, kv_width), BF16), vmem((rows, kv_width), BF16),
        vmem((kv_heads, *packed), F32), vmem((n, kv_heads, *packed), BF16),
        vmem((rows, q_width), F32),
        vmem((kv_heads, stack, LANES), BF16), vmem((kv_heads, stack, LANES), BF16),
        vmem((dp, rows, share), BF16), vmem((share, dp * rows), BF16),
        vmem((dp, share, kv_width), BF16), vmem((dp, share, kv_width), BF16),
        vmem((rows, q_width), F32),
        vmem((kv_heads, n, *packed), BF16),
        vmem((kv_heads, 2, *packed), BF16), vmem((kv_heads, 2, *packed), BF16),
        vmem((kv_heads, 3, *packed), BF16),
        vmem((kv_heads, dp, *packed), BF16),
        vmem((rows, kv_width), BF16), vmem((rows, kv_width), BF16),
        vmem((kv_heads, 2, share // 2, LANES), BF16),
        vmem((kv_heads, 2 * n, share // 2, LANES), BF16),
        vmem((kv_heads, 2, share // 2, LANES), BF16), vmem((kv_heads, share // 2, LANES), BF16),
        dma((11,)), dma((2 + n,)), dma((n, kv_heads)), dma((2,)), dma((3,)), dma((3, 2)),
        dma((1,)), dma((kv_heads, 2)), dma((kv_heads,)),
        dma((2,)), dma((kv_heads,)), dma((kv_heads,)),
        dma((4,)), dma((kv_heads, 2)), dma((kv_heads,)),
    ]
    hbm = pl.BlockSpec(memory_space=pltpu.HBM)
    here = pl.BlockSpec(memory_space=pltpu.VMEM)
    results = [
        ((rows, width), BF16), ((rows, q_width), BF16),
        ((share, kv_width), F32), ((share, kv_width), F32),
    ]
    held_bytes = 65536 + sum(a * b * jnp.dtype(kind).itemsize for (a, b), kind in results)
    held = pl.pallas_call(
        functools.partial(step_kernel, n, dp),
        out_shape=[pltpu.VMEM(shape, kind) for shape, kind in results],
        in_specs=[hbm] * 11,
        out_specs=[here] * 4,
        scratch_shapes=scratch,
        compiler_params=pltpu.CompilerParams(
            collective_id=0, has_side_effects=True, vmem_limit_bytes=VMEM_BYTES - held_bytes
        ),
    )(
        inputs[0], queries[0], keys[0], values[0], out_grad[0],
        query_gain[None], key_gain[None],
        key_matrix, value_matrix, jnp.asarray(cos_tab), jnp.asarray(sin_tab),
    )
    dx, dq, kw, vw = pl.pallas_call(
        write_kernel,
        out_shape=[jax.ShapeDtypeStruct(shape, kind) for shape, kind in results],
        in_specs=[here] * 4,
        out_specs=[hbm] * 4,
        scratch_shapes=[dma((4,))],
        compiler_params=pltpu.CompilerParams(vmem_limit_bytes=8 * 1024 * 1024),
    )(*held)
    return dx[None], dq[None], kw, vw


def device_step(inputs, *rest):
    n = lax.axis_size("sp")
    dp = lax.axis_size("dp")
    rows, width = inputs.shape[1:]
    fits = n == 4 and dp == 8 and width % (dp * LANES) == 0 and rows == LANES
    if fits and (width // dp) % (32 * n) == 0:
        return kernel_step(n, dp, inputs, *rest)
    return on_device(inputs, *rest)


def solution(mesh):
    return jax.shard_map(
        device_step,
        mesh=mesh,
        in_specs=(
            P("dp", "sp", None),
            P("dp", "sp", None),
            P("dp", "sp", None),
            P("dp", "sp", None),
            P("dp", "sp", None),
            P(),
            P(),
            P("dp", None),
            P("dp", None),
        ),
        out_specs=(P("dp", "sp", None), P("dp", "sp", None), P("dp", None), P("dp", None)),
        check_vma=False,
    )
```

```python
import functools

import jax
import jax.numpy as jnp
import numpy as np
from jax import lax
from jax.experimental import pallas as pl
from jax.experimental.pallas import tpu as pltpu
from jax.sharding import PartitionSpec as P

QUERY_HEADS = 16
KEY_VALUE_HEADS = 4
HEAD_CHANNELS = 64
GRID = 64


rope_base = 10000.0
norm_eps = 0.5
score_scale = 0.125


def product(pattern, first_op, second_op):
    return jnp.einsum(pattern, first_op, second_op, preferred_element_type=jnp.float32)


def rotary_tables(token_length):
    position = jnp.arange(token_length, dtype=jnp.int32)
    grid_row = (position // GRID).astype(jnp.float32)
    grid_col = (position % GRID).astype(jnp.float32)
    half_pairs = HEAD_CHANNELS // 4
    inv_freq = rope_base ** (-jnp.arange(half_pairs, dtype=jnp.float32) / half_pairs)
    angles = jnp.concatenate([grid_row[:, None] * inv_freq, grid_col[:, None] * inv_freq], axis=1)
    return (jnp.cos(angles), jnp.sin(angles))


def rotate(vector, cos_tab, sin_tab):
    even_part = vector[..., 0::2]
    odd_part = vector[..., 1::2]
    turned = jnp.stack(
        [even_part * cos_tab - odd_part * sin_tab, even_part * sin_tab + odd_part * cos_tab],
        axis=-1,
    )
    return turned.reshape(vector.shape)


def rotate_back(cotangent, cos_tab, sin_tab):
    even_part = cotangent[..., 0::2]
    odd_part = cotangent[..., 1::2]
    turned = jnp.stack(
        [even_part * cos_tab + odd_part * sin_tab, odd_part * cos_tab - even_part * sin_tab],
        axis=-1,
    )
    return turned.reshape(cotangent.shape)


def inverse_rms(vector):
    return lax.rsqrt(jnp.mean(vector * vector, axis=-1, keepdims=True) + norm_eps)


def norm_back(vector, inv_scale, cotangent, gain_vec):
    weighted = cotangent * gain_vec
    inner_mean = jnp.mean(weighted * vector, axis=-1, keepdims=True)
    return inv_scale * (weighted - vector * inv_scale * inv_scale * inner_mean)


def head_grads(
    query_in, key_input, value_input, grad_in, query_gain, key_gain, cos_tab, sin_tab, block_rows
):
    token_length, groups, per_group, head_dim = query_in.shape
    cos_four = cos_tab[:, None, None, :]
    sin_four = sin_tab[:, None, None, :]
    cos_three = cos_tab[:, None, :]
    sin_three = sin_tab[:, None, :]
    query_f = query_in.astype(jnp.float32)
    query_inv = inverse_rms(query_f)
    query_rot = rotate(query_f * query_inv * query_gain, cos_four, sin_four).astype(jnp.bfloat16)
    key_f = key_input.astype(jnp.float32)
    key_inv = inverse_rms(key_f)
    key_rot = rotate(key_f * key_inv * key_gain, cos_three, sin_three).astype(jnp.bfloat16)
    num_blocks = token_length // block_rows
    query_blocks = query_rot.reshape(num_blocks, block_rows, groups, per_group, head_dim)
    grad_blocks = grad_in.reshape(num_blocks, block_rows, groups, per_group, head_dim)

    def attend_block(carried, pieces):
        key_acc, value_acc = carried
        query_piece, grad_piece = pieces
        scores = product("qgrd,cgd->grqc", query_piece, key_rot) * score_scale
        row_max = jnp.max(scores, axis=-1, keepdims=True)
        shifted = jnp.exp(scores - row_max)
        attn_prob = shifted / jnp.sum(shifted, axis=-1, keepdims=True)
        prob_low = attn_prob.astype(jnp.bfloat16)
        prob_grad = product("qgrd,cgd->grqc", grad_piece, value_input)
        row_dot = jnp.sum(attn_prob * prob_grad, axis=-1, keepdims=True)
        score_grad = (attn_prob * (prob_grad - row_dot) * score_scale).astype(jnp.bfloat16)
        dq_piece = product("grqc,cgd->qgrd", score_grad, key_rot)
        key_acc = key_acc + product("grqc,qgrd->cgd", score_grad, query_piece)
        value_acc = value_acc + product("grqc,qgrd->cgd", prob_low, grad_piece)
        return ((key_acc, value_acc), dq_piece)

    empty_acc = jnp.zeros((token_length, groups, head_dim), jnp.float32)
    (key_rot_grad, value_acc), query_rot_grad = lax.scan(
        attend_block, (empty_acc, empty_acc), (query_blocks, grad_blocks)
    )
    query_rot_grad = query_rot_grad.reshape(token_length, groups, per_group, head_dim)
    query_grad = norm_back(
        query_f, query_inv, rotate_back(query_rot_grad, cos_four, sin_four), query_gain
    ).astype(jnp.bfloat16)
    key_portion = norm_back(
        key_f, key_inv, rotate_back(key_rot_grad, cos_three, sin_three), key_gain
    ).astype(jnp.bfloat16)
    return (query_grad, key_portion, value_acc.astype(jnp.bfloat16))


def on_device(
    inputs, queries, keys, values, out_grad, query_gain, key_gain, key_matrix, value_matrix
):
    sp_count = lax.axis_size("sp")
    dp_count = lax.axis_size("dp")
    token_row_block = inputs.shape[1]
    token_length = token_row_block * sp_count
    local_heads = QUERY_HEADS // sp_count
    portion_heads = min(local_heads, QUERY_HEADS // KEY_VALUE_HEADS)
    kv_here = local_heads // portion_heads
    group_copies = QUERY_HEADS // KEY_VALUE_HEADS // portion_heads
    key_value_width = KEY_VALUE_HEADS * HEAD_CHANNELS
    key_positions = jnp.repeat(
        keys[0].reshape(token_row_block, KEY_VALUE_HEADS, HEAD_CHANNELS), group_copies, axis=1
    ).reshape(token_row_block, key_value_width * group_copies)
    value_positions = jnp.repeat(
        values[0].reshape(token_row_block, KEY_VALUE_HEADS, HEAD_CHANNELS), group_copies, axis=1
    ).reshape(token_row_block, key_value_width * group_copies)
    grad_heads, query_heads, key_heads, value_heads = (
        lax.all_to_all(out_grad[0], "sp", split_axis=1, concat_axis=0, tiled=True),
        lax.all_to_all(queries[0], "sp", split_axis=1, concat_axis=0, tiled=True),
        lax.all_to_all(key_positions, "sp", split_axis=1, concat_axis=0, tiled=True),
        lax.all_to_all(value_positions, "sp", split_axis=1, concat_axis=0, tiled=True),
    )
    cos_tab, sin_tab = rotary_tables(token_length)
    query_part, key_portion, value_portion = head_grads(
        query_heads.reshape(token_length, kv_here, portion_heads, HEAD_CHANNELS),
        key_heads.reshape(token_length, kv_here, HEAD_CHANNELS),
        value_heads.reshape(token_length, kv_here, HEAD_CHANNELS),
        grad_heads.reshape(token_length, kv_here, portion_heads, HEAD_CHANNELS),
        query_gain,
        key_gain,
        cos_tab,
        sin_tab,
        min(512, token_length),
    )
    query_tokens, key_token_rows, value_token_rows = (
        lax.all_to_all(
            query_part.reshape(token_length, local_heads * HEAD_CHANNELS),
            "sp",
            split_axis=0,
            concat_axis=1,
            tiled=True,
        ),
        lax.all_to_all(
            key_portion.reshape(token_length, kv_here * HEAD_CHANNELS),
            "sp",
            split_axis=0,
            concat_axis=1,
            tiled=True,
        ),
        lax.all_to_all(
            value_portion.reshape(token_length, kv_here * HEAD_CHANNELS),
            "sp",
            split_axis=0,
            concat_axis=1,
            tiled=True,
        ),
    )
    key_gradient = (
        key_token_rows.reshape(token_row_block, KEY_VALUE_HEADS, group_copies, HEAD_CHANNELS)
        .astype(jnp.float32)
        .sum(axis=2)
        .astype(jnp.bfloat16)
    )
    value_gradient = (
        value_token_rows.reshape(token_row_block, KEY_VALUE_HEADS, group_copies, HEAD_CHANNELS)
        .astype(jnp.float32)
        .sum(axis=2)
        .astype(jnp.bfloat16)
    )
    projection_gradient = jnp.concatenate(
        [
            key_gradient.reshape(token_row_block, key_value_width),
            value_gradient.reshape(token_row_block, key_value_width),
        ],
        axis=1,
    )
    joined_weight = jnp.concatenate([key_matrix, value_matrix], axis=1)
    input_grad = lax.dot_general(
        projection_gradient,
        lax.all_gather(joined_weight, "dp", axis=0, tiled=True),
        (((1,), (1,)), ((), ())),
        preferred_element_type=jnp.float32,
    ).astype(jnp.bfloat16)
    token_in = inputs[0]
    width = inputs.shape[2]
    row_share = width // (sp_count * dp_count)
    permuted = (
        token_in.reshape(token_row_block, dp_count, sp_count, row_share)
        .transpose(0, 2, 1, 3)
        .reshape(token_row_block, width)
    )
    share_cols = lax.all_to_all(permuted, "sp", split_axis=1, concat_axis=0, tiled=True)
    all_grads = lax.all_gather(projection_gradient, "sp", axis=0, tiled=True)
    grad_piece = lax.psum_scatter(
        lax.dot_general(
            share_cols, all_grads, (((0,), (0,)), ((), ())), preferred_element_type=jnp.float32
        ).astype(jnp.bfloat16),
        "dp",
        scatter_dimension=0,
        tiled=True,
    ).astype(jnp.float32)
    weight_grad = lax.all_gather(grad_piece, "sp", axis=0, tiled=True)
    return (
        input_grad[None],
        query_tokens[None],
        weight_grad[:, :key_value_width],
        weight_grad[:, key_value_width:],
    )


LANES = 128
VMEM_BYTES = 67043328
MESH = pl.DeviceIdType.MESH
F32 = jnp.float32
BF16 = jnp.bfloat16


def pair_tables(token_length):
    position = np.arange(token_length)
    half_pairs = HEAD_CHANNELS // 4
    inv_freq = (rope_base ** (-np.arange(half_pairs) / half_pairs)).astype(np.float32)
    row = (position // GRID).astype(np.float32)
    col = (position % GRID).astype(np.float32)
    angles = np.concatenate([row[:, None] * inv_freq, col[:, None] * inv_freq], axis=1)
    cos_tab = np.repeat(np.cos(angles), 2, axis=1)
    sin_tab = np.repeat(np.sin(angles), 2, axis=1)
    sin_tab[:, 0::2] *= -1.0
    return (
        np.tile(cos_tab, (1, 2)).astype(np.float32),
        np.tile(sin_tab, (1, 2)).astype(np.float32),
    )


def swap_pairs(x):
    lane = lax.broadcasted_iota(jnp.int32, x.shape, 1)
    return jnp.where(lane % 2 == 0, pltpu.roll(x, LANES - 1, 1), pltpu.roll(x, 1, 1))


def head_mean(z):
    row = lax.broadcasted_iota(jnp.int32, (LANES, LANES), 0) // HEAD_CHANNELS
    col = lax.broadcasted_iota(jnp.int32, (LANES, LANES), 1) // HEAD_CHANNELS
    ones = jnp.where(row == col, 1.0, 0.0).astype(BF16)
    high = z.astype(BF16)
    low = (z - high.astype(F32)).astype(BF16)
    total = jnp.dot(high, ones, preferred_element_type=F32)
    total = total + jnp.dot(low, ones, preferred_element_type=F32)
    return total * (1.0 / HEAD_CHANNELS)


def norm_rotate(x, gain, cos_tab, sin_tab):
    inv = lax.rsqrt(head_mean(x * x) + norm_eps)
    y = x * inv * gain
    return y * cos_tab + swap_pairs(y) * sin_tab, inv


def norm_rotate_back(x, inv, cotangent, gain, cos_tab, sin_tab):
    turned = cotangent * cos_tab - swap_pairs(cotangent) * sin_tab
    weighted = turned * gain
    return inv * (weighted - x * (inv * inv * head_mean(weighted * x)))


def contract(a, b, dims):
    return lax.dot_general(a, b, (dims, ((), ())), preferred_element_type=F32)


def step_kernel(
    n, dp,
    x_hbm, q_hbm, k_hbm, v_hbm, do_hbm, qg_hbm, kg_hbm, km_hbm, vm_hbm, cos_hbm, sin_hbm,
    dx_buf, dq_buf, kw_buf, vw_buf,
    qg_ref, kg_ref, q_buf, do_buf, cos_buf, sin_buf, k_own, v_own, k_head, k_inv, kv_all, q_inv, q_st, do_st,
    x_all, x_t, wk_all, wv_all, dq_acc, part, comb_in, comb, got, g_all, own_k, own_v,
    wg_part, wg_got, fin_all, fin_low,
    ready, local_sem, kv_send, kv_recv, x_sem, w_send, w_recv, p_send, c_recv, p_recv,
    g_send, gd_recv, gm_recv, r_send, r_recv, f_recv,
):
    me = lax.axis_index("sp")
    md = lax.axis_index("dp")
    rows, q_width = q_buf.shape
    heads = kv_all.shape[1]
    share = x_all.shape[2]
    per_group = q_width // (heads * HEAD_CHANNELS)
    half_share = share // 2
    mate = md + 1 - 2 * (md % 2)
    last = n - 1
    first_mid = n // 2 - 1
    partner = me + 1 - 2 * (me % 2)
    low_side = me < n // 2
    other_end = jnp.where(low_side, last, 0)
    other_mid = jnp.where(low_side, n // 2, n // 2 - 1)
    is_end = jnp.logical_or(me == 0, me == last)
    near_chips = dp // 2 - 1
    core = md % 2
    upper = md + 1 - core
    side_mid = jnp.where(is_end, partner, me)
    is_owner = jnp.logical_and(jnp.logical_not(is_end), core == 1)
    first_straight = 0
    relayed = 1

    def sp_peer(o):
        return lax.rem(me + o, n)

    def sp_from(o):
        return lax.rem(me - o + n, n)

    def dp_peer(o):
        return lax.rem(md + o, dp)

    def dp_from(o):
        return lax.rem(md - o + dp, dp)

    def mate_from(o):
        return lax.rem(mate - o + dp, dp)

    def pair(c):
        return pl.ds(c * LANES, LANES)

    def columns(d):
        return pl.ds(pl.multiple_of(d * share, share), share)

    barrier = pltpu.get_barrier_semaphore()

    def greet(where):
        pl.semaphore_signal(barrier, inc=1, device_id=where, device_id_type=MESH)

    @pl.when(me > 0)
    def _():
        greet({"sp": me - 1})

    @pl.when(me < last)
    def _():
        greet({"sp": me + 1})

    @pl.when(jnp.logical_not(is_end))
    def _():
        greet({"sp": other_end})

    def flip(bit):
        return md + bit - 2 * bit * ((md // bit) % 2)

    x_side, y_side = flip(2), flip(4)
    corner = x_side + y_side - md
    beside = [mate]
    for d in (x_side, y_side):
        beside += [d, d + mate - md]
    for d in beside:
        greet({"dp": d})

    my_rows = pl.ds(pl.multiple_of(me * rows, rows), rows)
    wanted = [
        (k_hbm, k_own), (v_hbm, v_own), (cos_hbm.at[my_rows, :], cos_buf),
        (sin_hbm.at[my_rows, :], sin_buf), (kg_hbm, kg_ref), (qg_hbm, qg_ref),
        (q_hbm, q_buf), (do_hbm, do_buf),
        (x_hbm.at[:, columns(md)], x_all.at[md]), (km_hbm, wk_all.at[md]), (vm_hbm, wv_all.at[md]),
    ]
    local = [
        pltpu.make_async_copy(src, dst, local_sem.at[i]) for i, (src, dst) in enumerate(wanted)
    ]
    for copy in local:
        copy.start()

    def remote(src, dst, send, recv, where):
        return pltpu.make_async_remote_copy(
            src_ref=src, dst_ref=dst, send_sem=send, recv_sem=recv,
            device_id=where, device_id_type=MESH,
        )

    def send(*args):
        remote(*args).start()

    def arrived(dst, recv):
        remote(dst, dst, recv, recv, {"sp": me}).wait_recv()

    def departed(src, sem):
        remote(src, src, sem, sem, {"sp": me}).wait_send()

    low_lanes = lax.broadcasted_iota(jnp.int32, (rows, LANES), 1) < HEAD_CHANNELS

    def shift(a):
        return pltpu.roll(a, HEAD_CHANNELS, 1)

    with jax.named_scope("local"):
        for copy in local[:6]:
            copy.wait()
    cos_own = cos_buf[...]
    sin_own = sin_buf[...]
    q_gain = jnp.concatenate([qg_ref[...], qg_ref[...]], axis=1)
    k_gain = jnp.concatenate([kg_ref[...], kg_ref[...]], axis=1)

    for c in range(heads // 2):
        keys = k_own[:, pair(c)].astype(F32)
        vals = v_own[:, pair(c)].astype(F32)
        turned, inv = norm_rotate(keys, k_gain, cos_own, sin_own)
        kv_all[me, 2 * c] = jnp.where(low_lanes, turned, shift(vals)).astype(BF16)
        kv_all[me, 2 * c + 1] = jnp.where(low_lanes, shift(turned), vals).astype(BF16)
        k_head[2 * c] = keys
        k_head[2 * c + 1] = shift(keys)
        k_inv[2 * c] = inv
        k_inv[2 * c + 1] = shift(inv)

    with jax.named_scope("barrier"):
        pl.semaphore_wait(barrier, 2 + len(beside))

    def send_kv(src, g, sem, where):
        block = kv_all.at[src, g]
        send(block, block, kv_send.at[sem], kv_recv.at[src, g], {"sp": where})

    for g in range(heads):
        send_kv(me, g, 0, other_mid)
        send_kv(me, g, 1, partner)

    pl.semaphore_signal(ready, inc=1, device_id={"dp": x_side}, device_id_type=MESH)

    def send_tokens(peers):
        for d in peers:
            send(x_hbm.at[:, columns(d)], x_all.at[md], x_sem.at[0], x_sem.at[1], {"dp": d})

    send_tokens(beside)

    top = pl.ds(0, half_share)
    bottom = pl.ds(half_share, half_share)
    full = pl.ds(0, share)
    weights = [(km_hbm, wk_all, full), (vm_hbm, wv_all, top), (vm_hbm, wv_all, bottom)]

    def send_weights(kind, peers):
        src, dst, at = weights[kind]
        for d in peers:
            send(src.at[at], dst.at[md, at], w_send.at[kind],
                 w_recv.at[kind, 1 if d is mate else 0], {"dp": d})

    def pass_weights(kind):
        _, dst, at = weights[kind]
        arrived(dst.at[pl.ds(0, near_chips), at], w_recv.at[kind, 0])
        for o in range(2, dp, 2):
            block = dst.at[dp_from(o), at]
            send(block, block, w_send.at[kind], w_recv.at[kind, 1], {"dp": mate})

    def finish_weights(kind):
        _, dst, at = weights[kind]
        arrived(dst.at[pl.ds(0, dp // 2), at], w_recv.at[kind, 1])

    for kind in range(2):
        send_weights(kind, (x_side, y_side, mate))

    with jax.named_scope("local2"):
        for copy in local[6:8]:
            copy.wait()
    with jax.named_scope("qrot"):
        for c in range(q_width // LANES):
            turned, inv = norm_rotate(q_buf[:, pair(c)].astype(F32), q_gain, cos_own, sin_own)
            q_inv[:, pair(c)] = inv
            turned = turned * score_scale
            grads = do_buf[:, pair(c)].astype(F32)
            g, r = divmod(2 * c, per_group)
            for a, (query, grad) in enumerate([(turned, shift(grads)), (shift(turned), grads)]):
                to = pl.ds((r + a) * rows, rows)
                q_st[g, to, :] = jnp.where(low_lanes, query, 0.0).astype(BF16)
                do_st[g, to, :] = jnp.where(low_lanes, 0.0, grad).astype(BF16)

    pl.semaphore_wait(ready, 1)
    send_tokens((corner, corner + mate - md))
    for kind in range(2):
        send_weights(kind, (corner,))

    def take_kv(src, g):
        arrived(kv_all.at[src, g], kv_recv.at[src, g])

    def relay(src, g, where):
        take_kv(src, g)
        send_kv(src, g, 2 + src, where)

    def relays(turns):
        @pl.when(jnp.logical_not(is_end))
        def _():
            for src, g in turns:
                relay([other_mid, other_end][src], g, partner)

    turns = sorted(
        [(0, g) for g in range(heads)] + [(1, g) for g in range(heads)],
        key=lambda turn: turn[1] + 0.5 * turn[0],
    )
    with jax.named_scope("relay"):
        relays(turns)

    step = 1

    def attend(g):
        kv = kv_all[:, g].reshape(n * rows, LANES)
        both = None
        score_grads = []
        for r in range(0, per_group, step):
            at = pl.ds(r * rows, step * rows)
            queries = q_st[g, at, :]
            grads = do_st[g, at, :]
            scores = contract(kv, queries, ((1,), (1,)))
            prob_grad = contract(kv, grads, ((1,), (1,)))
            shifted = jnp.exp(scores - jnp.max(scores, axis=0, keepdims=True))
            inverse = 1.0 / jnp.sum(shifted, axis=0, keepdims=True)
            prob = shifted * inverse
            row_dot = jnp.sum(prob * prob_grad, axis=0, keepdims=True)
            score_grad = (prob * (prob_grad - row_dot)).astype(BF16)
            term = contract(score_grad, queries, ((1,), (0,)))
            term = term + contract(prob.astype(BF16), grads, ((1,), (0,)))
            both = term if both is None else both + term
            score_grads.append(score_grad)
        part[g] = both.astype(BF16).reshape(n, rows, LANES)
        return kv, score_grads

    def query_part(g, kv, score_grads):
        parts = [contract(kv[:, :HEAD_CHANNELS], a, ((0,), (0,))) for a in score_grads]
        for r in range(0, per_group, 2):
            head = g * per_group + r
            dq_acc[:, head * HEAD_CHANNELS:head * HEAD_CHANNELS + LANES] = jnp.concatenate(
                [parts[r], parts[r + 1]], axis=0
            ).T

    def straight(g):
        return core == 0 if g >= first_straight else core < 0

    def send_parts(g):
        @pl.when(straight(g))
        def _():
            for where in (other_end, other_mid):
                send(part.at[g, where], got.at[g, jnp.where(is_end, 1, 2)], p_send.at[0],
                     p_recv.at[g], {"sp": where})

        @pl.when(jnp.logical_and(is_end, jnp.logical_not(straight(g))))
        def _():
            for i, where in enumerate([other_end, other_mid]):
                send(part.at[g, where], comb_in.at[g, i], p_send.at[0], c_recv.at[g, i],
                     {"sp": partner})

        send(part.at[g, partner], got.at[g, 0], p_send.at[0], p_recv.at[g], {"sp": partner})

    def combine(g):
        @pl.when(jnp.logical_not(jnp.logical_or(is_end, straight(g))))
        def _():
            for i, where in enumerate([other_end, other_mid]):
                arrived(comb_in.at[g, i], c_recv.at[g, i])
                total = comb_in[g, i].astype(F32) + part[g, where].astype(F32)
                comb[g, i] = total.astype(BF16)
                send(comb.at[g, i], got.at[g, 1], p_send.at[0], p_recv.at[g], {"sp": where})

    def own_grads(g):
        with jax.named_scope(f"gotwait{g}"):
            @pl.when(straight(g))
            def _():
                arrived(got.at[g], p_recv.at[g])

            @pl.when(jnp.logical_not(straight(g)))
            def _():
                arrived(got.at[g, pl.ds(0, 2)], p_recv.at[g])
        total = part[g, me].astype(F32) + got[g, 0].astype(F32) + got[g, 1].astype(F32)
        total = total + jnp.where(straight(g), got[g, 2].astype(F32), 0.0)
        keys = k_head[g]
        back = norm_rotate_back(keys, k_inv[g], total, k_gain, cos_own, sin_own)
        both = jnp.where(low_lanes, back, total).astype(BF16)
        g_all[g, md] = both
        mine = g_all.at[g, md]
        for o in range(2, dp, 2):
            send(mine, mine, g_send.at[0], gd_recv.at[g], {"dp": dp_peer(o)})
        send(mine, mine, g_send.at[0], gm_recv.at[g], {"dp": mate})
        at = slice(g * HEAD_CHANNELS, (g + 1) * HEAD_CHANNELS)
        own_k[:, at] = both[:, :HEAD_CHANNELS]
        own_v[:, at] = both[:, HEAD_CHANNELS:]

    def pass_on(g):
        with jax.named_scope(f"gdwait{g}"):
            arrived(g_all.at[g, pl.ds(0, near_chips)], gd_recv.at[g])
        for o in range(2, dp, 2):
            block = g_all.at[g, dp_from(o)]
            send(block, block, g_send.at[1], gm_recv.at[g], {"dp": mate})

    def weight_grads(g):
        with jax.named_scope(f"gmwait{g}"):
            arrived(g_all.at[g, pl.ds(0, dp // 2)], gm_recv.at[g])
        total = contract(x_t[...], g_all[g].reshape(dp * rows, LANES), ((1,), (0,)))
        wg_part[g] = total.astype(BF16).reshape(2, half_share, LANES)

        def give(half, where):
            send(wg_part.at[g, half], wg_got.at[g, core * n + me], r_send.at[0],
                 r_recv.at[g, core], {"sp": where, "dp": upper})

        give(other_mid - first_mid, other_mid)

        @pl.when(jnp.logical_not(is_owner))
        def _():
            give(side_mid - first_mid, side_mid)

    def sum_weight_grads(g):
        @pl.when(is_owner)
        def _():
            mine = me - first_mid
            with jax.named_scope(f"rwait{g}"):
                arrived(wg_got.at[g, pl.ds(0, last)], r_recv.at[g, 1])
            total = wg_part[g, mine].astype(F32)
            for o in range(1, n):
                total = total + wg_got[g, n + sp_from(o)].astype(F32)
            fin_all[g, mine] = total.astype(BF16)
            with jax.named_scope(f"rwaits{g}"):
                arrived(wg_got.at[g, pl.ds(0, n)], r_recv.at[g, 0])
            total = wg_got[g, 0].astype(F32)
            for src in range(1, n):
                total = total + wg_got[g, src].astype(F32)
            fin_low[g] = total.astype(BF16)
            for block, d in ((fin_low.at[g], mate), (fin_all.at[g, mine], md)):
                if g >= relayed:
                    send(block, fin_all.at[g, mine], r_send.at[3], f_recv.at[g],
                         {"sp": other_end, "dp": d})
                for where in (partner, other_mid):
                    send(block, fin_all.at[g, mine], r_send.at[1], f_recv.at[g],
                         {"sp": where, "dp": d})
            send(fin_low.at[g], fin_all.at[g, mine], r_send.at[1], f_recv.at[g], {"dp": mate})

    def hand_on(g):
        block = fin_all.at[g, other_mid - first_mid]
        send(block, block, r_send.at[2], f_recv.at[g], {"sp": partner})

    def relay_weight_grads(g):
        @pl.when(is_owner)
        def _():
            arrived(fin_all.at[g, 0], f_recv.at[g])
            hand_on(g)

    def put_weight_grads(g):
        with jax.named_scope(f"fwait{g}"):
            if g >= relayed:
                @pl.when(is_owner)
                def _():
                    arrived(fin_all.at[g, 0], f_recv.at[g])

            @pl.when(jnp.logical_not(is_owner))
            def _():
                arrived(fin_all.at[g], f_recv.at[g])
        if g < relayed:
            @pl.when(jnp.logical_not(jnp.logical_or(is_end, is_owner)))
            def _():
                hand_on(g)
        total = fin_all[g].reshape(share, LANES).astype(F32)
        at = slice(g * HEAD_CHANNELS, (g + 1) * HEAD_CHANNELS)
        kw_buf[:, at] = total[:, :HEAD_CHANNELS]
        vw_buf[:, at] = total[:, HEAD_CHANNELS:]

    def query_grads(c):
        dq_buf[:, pair(c)] = norm_rotate_back(
            q_buf[:, pair(c)].astype(F32), q_inv[:, pair(c)], dq_acc[:, pair(c)],
            q_gain * score_scale, cos_own, sin_own,
        ).astype(BF16)

    def project(src):
        out = contract(own_k[...], wk_all[src], ((1,), (1,)))
        out = out + contract(own_v[...], wv_all[src], ((1,), (1,)))
        dx_buf[:, columns(src)] = out.astype(BF16)

    blocks = q_width // LANES
    for g in range(heads):
        with jax.named_scope(f"kvwait{g}"):
            take_kv(partner, g)

            @pl.when(is_end)
            def _():
                take_kv(other_mid, g)
                take_kv(other_end, g)
        if g == heads - 1:
            with jax.named_scope("comb0"):
                combine(0)
        with jax.named_scope(f"attend{g}"):
            kept = attend(g)
            send_parts(g)
            query_part(g, *kept)
    def scoped(name, step, *args):
        with jax.named_scope(name):
            step(*args)

    def query_half(first):
        for c in range(first, first + blocks // 2):
            query_grads(c)

    scoped("comb1", combine, 1)
    scoped("comb2", combine, 2)
    scoped("comb3", combine, 3)
    scoped("dqa", query_half, 0)
    scoped("own0", own_grads, 0)
    scoped("own1", own_grads, 1)
    with jax.named_scope("xt"):
        for copy in local[8:]:
            copy.wait()
        arrived(x_all.at[pl.ds(0, dp - 1)], x_sem.at[1])
        for src in range(dp):
            x_t[:, src * rows:(src + 1) * rows] = x_all[src].T
    scoped("own2", own_grads, 2)
    scoped("pass0", pass_on, 0)
    scoped("own3", own_grads, 3)
    send_weights(2, (x_side, y_side, corner, mate))
    scoped("dqb", query_half, blocks // 2)
    with jax.named_scope("wpass"):
        pass_weights(0)
        pass_weights(1)
    scoped("wg0", weight_grads, 0)
    scoped("pass1", pass_on, 1)
    scoped("wg1", weight_grads, 1)
    scoped("pass2", pass_on, 2)
    scoped("pass3", pass_on, 3)
    scoped("sum0", sum_weight_grads, 0)
    scoped("wg2", weight_grads, 2)
    scoped("wg3", weight_grads, 3)
    scoped("sum1", sum_weight_grads, 1)
    scoped("wlate", pass_weights, 2)
    with jax.named_scope("proja"):
        for o in range(0, dp, 2):
            project(dp_from(o))
    scoped("hand0", relay_weight_grads, 0)
    scoped("sum2", sum_weight_grads, 2)
    scoped("sum3", sum_weight_grads, 3)
    with jax.named_scope("wfin"):
        for kind in range(3):
            finish_weights(kind)
    with jax.named_scope("projb"):
        for o in range(0, dp, 2):
            project(mate_from(o))
    for g in range(heads):
        scoped(f"put{g}", put_weight_grads, g)

    with jax.named_scope("drain"):
        departed(kv_all.at[me], kv_send.at[0])
        departed(kv_all.at[me], kv_send.at[1])

        @pl.when(jnp.logical_not(is_end))
        def _():
            departed(kv_all.at[other_mid], kv_send.at[2 + other_mid])
            departed(kv_all.at[other_end], kv_send.at[2 + other_end])

        departed(x_all.at[pl.ds(0, dp - 1)], x_sem.at[0])
        for kind, (_, dst, at) in enumerate(weights):
            departed(dst.at[pl.ds(0, dp - 1), at], w_send.at[kind])
        departed(part.at[:, pl.ds(0, 3)], p_send.at[0])
        departed(g_all.at[:, pl.ds(0, dp // 2)], g_send.at[0])
        departed(g_all.at[:, pl.ds(0, near_chips)], g_send.at[1])

        @pl.when(is_owner)
        def _():
            departed(wg_part.at[:, 0], r_send.at[0])
            departed(wg_got.at[:, pl.ds(0, 5)], r_send.at[1])
            departed(wg_got.at[pl.ds(0, heads - relayed), pl.ds(0, 2)], r_send.at[3])

        @pl.when(jnp.logical_not(is_owner))
        def _():
            departed(wg_part, r_send.at[0])

        @pl.when(jnp.logical_not(is_end))
        def _():
            departed(fin_low.at[pl.ds(0, relayed)], r_send.at[2])


def write_kernel(*refs):
    count = (len(refs) - 1) // 2
    copies = [
        pltpu.make_async_copy(refs[i], refs[count + i], refs[-1].at[i]) for i in range(count)
    ]
    for copy in copies:
        copy.start()
    for copy in copies:
        copy.wait()


def kernel_step(
    n, dp, inputs, queries, keys, values, out_grad, query_gain, key_gain, key_matrix, value_matrix
):
    rows, width = inputs.shape[1:]
    q_width = queries.shape[2]
    kv_width = keys.shape[2]
    length = rows * n
    share = width // dp
    kv_heads = kv_width // HEAD_CHANNELS
    stack = rows * (q_width // kv_width)
    cos_tab, sin_tab = pair_tables(length)
    vmem = pltpu.VMEM
    dma = pltpu.SemaphoreType.DMA
    packed = (rows, LANES)
    scratch = [
        vmem((1, HEAD_CHANNELS), F32), vmem((1, HEAD_CHANNELS), F32),
        vmem((rows, q_width), BF16), vmem((rows, q_width), BF16),
        vmem(packed, F32), vmem(packed, F32),
        vmem((rows, kv_width), BF16), vmem((rows, kv_width), BF16),
        vmem((kv_heads, *packed), F32), vmem((kv_heads, *packed), F32),
        vmem((n, kv_heads, *packed), BF16),
        vmem((rows, q_width), F32),
        vmem((kv_heads, stack, LANES), BF16), vmem((kv_heads, stack, LANES), BF16),
        vmem((dp, rows, share), BF16), vmem((share, dp * rows), BF16),
        vmem((dp, share, kv_width), BF16), vmem((dp, share, kv_width), BF16),
        vmem((rows, q_width), F32),
        vmem((kv_heads, n, *packed), BF16),
        vmem((kv_heads, 2, *packed), BF16), vmem((kv_heads, 2, *packed), BF16),
        vmem((kv_heads, 3, *packed), BF16),
        vmem((kv_heads, dp, *packed), BF16),
        vmem((rows, kv_width), BF16), vmem((rows, kv_width), BF16),
        vmem((kv_heads, 2, share // 2, LANES), BF16),
        vmem((kv_heads, 2 * n, share // 2, LANES), BF16),
        vmem((kv_heads, 2, share // 2, LANES), BF16), vmem((kv_heads, share // 2, LANES), BF16),
        pltpu.SemaphoreType.REGULAR, dma((11,)), dma((2 + n,)), dma((n, kv_heads)), dma((2,)), dma((3,)), dma((3, 2)),
        dma((1,)), dma((kv_heads, 2)), dma((kv_heads,)),
        dma((2,)), dma((kv_heads,)), dma((kv_heads,)),
        dma((4,)), dma((kv_heads, 2)), dma((kv_heads,)),
    ]
    hbm = pl.BlockSpec(memory_space=pltpu.HBM)
    here = pl.BlockSpec(memory_space=pltpu.VMEM)
    results = [
        ((rows, width), BF16), ((rows, q_width), BF16),
        ((share, kv_width), F32), ((share, kv_width), F32),
    ]
    held_bytes = 65536 + sum(a * b * jnp.dtype(kind).itemsize for (a, b), kind in results)
    held = pl.pallas_call(
        functools.partial(step_kernel, n, dp),
        out_shape=[pltpu.VMEM(shape, kind) for shape, kind in results],
        in_specs=[hbm] * 11,
        out_specs=[here] * 4,
        scratch_shapes=scratch,
        compiler_params=pltpu.CompilerParams(
            collective_id=0, has_side_effects=True, vmem_limit_bytes=VMEM_BYTES - held_bytes
        ),
    )(
        inputs[0], queries[0], keys[0], values[0], out_grad[0],
        query_gain[None], key_gain[None],
        key_matrix, value_matrix, jnp.asarray(cos_tab), jnp.asarray(sin_tab),
    )
    dx, dq, kw, vw = pl.pallas_call(
        write_kernel,
        out_shape=[jax.ShapeDtypeStruct(shape, kind) for shape, kind in results],
        in_specs=[here] * 4,
        out_specs=[hbm] * 4,
        scratch_shapes=[dma((4,))],
        compiler_params=pltpu.CompilerParams(vmem_limit_bytes=8 * 1024 * 1024),
    )(*held)
    return dx[None], dq[None], kw, vw


def device_step(inputs, *rest):
    n = lax.axis_size("sp")
    dp = lax.axis_size("dp")
    rows, width = inputs.shape[1:]
    fits = n == 4 and dp == 8 and width % (dp * LANES) == 0 and rows == LANES
    if fits and (width // dp) % (32 * n) == 0:
        return kernel_step(n, dp, inputs, *rest)
    return on_device(inputs, *rest)


def solution(mesh):
    return jax.shard_map(
        device_step,
        mesh=mesh,
        in_specs=(
            P("dp", "sp", None),
            P("dp", "sp", None),
            P("dp", "sp", None),
            P("dp", "sp", None),
            P("dp", "sp", None),
            P(),
            P(),
            P("dp", None),
            P("dp", None),
        ),
        out_specs=(P("dp", "sp", None), P("dp", "sp", None), P("dp", None), P("dp", None)),
        check_vma=False,
    )
```

```python
import functools

import jax
import jax.numpy as jnp
import numpy as np
from jax import lax
from jax.experimental import pallas as pl
from jax.experimental.pallas import tpu as pltpu
from jax.sharding import PartitionSpec as P

QUERY_HEADS = 16
KEY_VALUE_HEADS = 4
HEAD_CHANNELS = 64
GRID = 64


rope_base = 10000.0
norm_eps = 0.5
score_scale = 0.125


def product(pattern, first_op, second_op):
    return jnp.einsum(pattern, first_op, second_op, preferred_element_type=jnp.float32)


def rotary_tables(token_length):
    position = jnp.arange(token_length, dtype=jnp.int32)
    grid_row = (position // GRID).astype(jnp.float32)
    grid_col = (position % GRID).astype(jnp.float32)
    half_pairs = HEAD_CHANNELS // 4
    inv_freq = rope_base ** (-jnp.arange(half_pairs, dtype=jnp.float32) / half_pairs)
    angles = jnp.concatenate([grid_row[:, None] * inv_freq, grid_col[:, None] * inv_freq], axis=1)
    return (jnp.cos(angles), jnp.sin(angles))


def rotate(vector, cos_tab, sin_tab):
    even_part = vector[..., 0::2]
    odd_part = vector[..., 1::2]
    turned = jnp.stack(
        [even_part * cos_tab - odd_part * sin_tab, even_part * sin_tab + odd_part * cos_tab],
        axis=-1,
    )
    return turned.reshape(vector.shape)


def rotate_back(cotangent, cos_tab, sin_tab):
    even_part = cotangent[..., 0::2]
    odd_part = cotangent[..., 1::2]
    turned = jnp.stack(
        [even_part * cos_tab + odd_part * sin_tab, odd_part * cos_tab - even_part * sin_tab],
        axis=-1,
    )
    return turned.reshape(cotangent.shape)


def inverse_rms(vector):
    return lax.rsqrt(jnp.mean(vector * vector, axis=-1, keepdims=True) + norm_eps)


def norm_back(vector, inv_scale, cotangent, gain_vec):
    weighted = cotangent * gain_vec
    inner_mean = jnp.mean(weighted * vector, axis=-1, keepdims=True)
    return inv_scale * (weighted - vector * inv_scale * inv_scale * inner_mean)


def head_grads(
    query_in, key_input, value_input, grad_in, query_gain, key_gain, cos_tab, sin_tab, block_rows
):
    token_length, groups, per_group, head_dim = query_in.shape
    cos_four = cos_tab[:, None, None, :]
    sin_four = sin_tab[:, None, None, :]
    cos_three = cos_tab[:, None, :]
    sin_three = sin_tab[:, None, :]
    query_f = query_in.astype(jnp.float32)
    query_inv = inverse_rms(query_f)
    query_rot = rotate(query_f * query_inv * query_gain, cos_four, sin_four).astype(jnp.bfloat16)
    key_f = key_input.astype(jnp.float32)
    key_inv = inverse_rms(key_f)
    key_rot = rotate(key_f * key_inv * key_gain, cos_three, sin_three).astype(jnp.bfloat16)
    num_blocks = token_length // block_rows
    query_blocks = query_rot.reshape(num_blocks, block_rows, groups, per_group, head_dim)
    grad_blocks = grad_in.reshape(num_blocks, block_rows, groups, per_group, head_dim)

    def attend_block(carried, pieces):
        key_acc, value_acc = carried
        query_piece, grad_piece = pieces
        scores = product("qgrd,cgd->grqc", query_piece, key_rot) * score_scale
        row_max = jnp.max(scores, axis=-1, keepdims=True)
        shifted = jnp.exp(scores - row_max)
        attn_prob = shifted / jnp.sum(shifted, axis=-1, keepdims=True)
        prob_low = attn_prob.astype(jnp.bfloat16)
        prob_grad = product("qgrd,cgd->grqc", grad_piece, value_input)
        row_dot = jnp.sum(attn_prob * prob_grad, axis=-1, keepdims=True)
        score_grad = (attn_prob * (prob_grad - row_dot) * score_scale).astype(jnp.bfloat16)
        dq_piece = product("grqc,cgd->qgrd", score_grad, key_rot)
        key_acc = key_acc + product("grqc,qgrd->cgd", score_grad, query_piece)
        value_acc = value_acc + product("grqc,qgrd->cgd", prob_low, grad_piece)
        return ((key_acc, value_acc), dq_piece)

    empty_acc = jnp.zeros((token_length, groups, head_dim), jnp.float32)
    (key_rot_grad, value_acc), query_rot_grad = lax.scan(
        attend_block, (empty_acc, empty_acc), (query_blocks, grad_blocks)
    )
    query_rot_grad = query_rot_grad.reshape(token_length, groups, per_group, head_dim)
    query_grad = norm_back(
        query_f, query_inv, rotate_back(query_rot_grad, cos_four, sin_four), query_gain
    ).astype(jnp.bfloat16)
    key_portion = norm_back(
        key_f, key_inv, rotate_back(key_rot_grad, cos_three, sin_three), key_gain
    ).astype(jnp.bfloat16)
    return (query_grad, key_portion, value_acc.astype(jnp.bfloat16))


def on_device(
    inputs, queries, keys, values, out_grad, query_gain, key_gain, key_matrix, value_matrix
):
    sp_count = lax.axis_size("sp")
    dp_count = lax.axis_size("dp")
    token_row_block = inputs.shape[1]
    token_length = token_row_block * sp_count
    local_heads = QUERY_HEADS // sp_count
    portion_heads = min(local_heads, QUERY_HEADS // KEY_VALUE_HEADS)
    kv_here = local_heads // portion_heads
    group_copies = QUERY_HEADS // KEY_VALUE_HEADS // portion_heads
    key_value_width = KEY_VALUE_HEADS * HEAD_CHANNELS
    key_positions = jnp.repeat(
        keys[0].reshape(token_row_block, KEY_VALUE_HEADS, HEAD_CHANNELS), group_copies, axis=1
    ).reshape(token_row_block, key_value_width * group_copies)
    value_positions = jnp.repeat(
        values[0].reshape(token_row_block, KEY_VALUE_HEADS, HEAD_CHANNELS), group_copies, axis=1
    ).reshape(token_row_block, key_value_width * group_copies)
    grad_heads, query_heads, key_heads, value_heads = (
        lax.all_to_all(out_grad[0], "sp", split_axis=1, concat_axis=0, tiled=True),
        lax.all_to_all(queries[0], "sp", split_axis=1, concat_axis=0, tiled=True),
        lax.all_to_all(key_positions, "sp", split_axis=1, concat_axis=0, tiled=True),
        lax.all_to_all(value_positions, "sp", split_axis=1, concat_axis=0, tiled=True),
    )
    cos_tab, sin_tab = rotary_tables(token_length)
    query_part, key_portion, value_portion = head_grads(
        query_heads.reshape(token_length, kv_here, portion_heads, HEAD_CHANNELS),
        key_heads.reshape(token_length, kv_here, HEAD_CHANNELS),
        value_heads.reshape(token_length, kv_here, HEAD_CHANNELS),
        grad_heads.reshape(token_length, kv_here, portion_heads, HEAD_CHANNELS),
        query_gain,
        key_gain,
        cos_tab,
        sin_tab,
        min(512, token_length),
    )
    query_tokens, key_token_rows, value_token_rows = (
        lax.all_to_all(
            query_part.reshape(token_length, local_heads * HEAD_CHANNELS),
            "sp",
            split_axis=0,
            concat_axis=1,
            tiled=True,
        ),
        lax.all_to_all(
            key_portion.reshape(token_length, kv_here * HEAD_CHANNELS),
            "sp",
            split_axis=0,
            concat_axis=1,
            tiled=True,
        ),
        lax.all_to_all(
            value_portion.reshape(token_length, kv_here * HEAD_CHANNELS),
            "sp",
            split_axis=0,
            concat_axis=1,
            tiled=True,
        ),
    )
    key_gradient = (
        key_token_rows.reshape(token_row_block, KEY_VALUE_HEADS, group_copies, HEAD_CHANNELS)
        .astype(jnp.float32)
        .sum(axis=2)
        .astype(jnp.bfloat16)
    )
    value_gradient = (
        value_token_rows.reshape(token_row_block, KEY_VALUE_HEADS, group_copies, HEAD_CHANNELS)
        .astype(jnp.float32)
        .sum(axis=2)
        .astype(jnp.bfloat16)
    )
    projection_gradient = jnp.concatenate(
        [
            key_gradient.reshape(token_row_block, key_value_width),
            value_gradient.reshape(token_row_block, key_value_width),
        ],
        axis=1,
    )
    joined_weight = jnp.concatenate([key_matrix, value_matrix], axis=1)
    input_grad = lax.dot_general(
        projection_gradient,
        lax.all_gather(joined_weight, "dp", axis=0, tiled=True),
        (((1,), (1,)), ((), ())),
        preferred_element_type=jnp.float32,
    ).astype(jnp.bfloat16)
    token_in = inputs[0]
    width = inputs.shape[2]
    row_share = width // (sp_count * dp_count)
    permuted = (
        token_in.reshape(token_row_block, dp_count, sp_count, row_share)
        .transpose(0, 2, 1, 3)
        .reshape(token_row_block, width)
    )
    share_cols = lax.all_to_all(permuted, "sp", split_axis=1, concat_axis=0, tiled=True)
    all_grads = lax.all_gather(projection_gradient, "sp", axis=0, tiled=True)
    grad_piece = lax.psum_scatter(
        lax.dot_general(
            share_cols, all_grads, (((0,), (0,)), ((), ())), preferred_element_type=jnp.float32
        ).astype(jnp.bfloat16),
        "dp",
        scatter_dimension=0,
        tiled=True,
    ).astype(jnp.float32)
    weight_grad = lax.all_gather(grad_piece, "sp", axis=0, tiled=True)
    return (
        input_grad[None],
        query_tokens[None],
        weight_grad[:, :key_value_width],
        weight_grad[:, key_value_width:],
    )


LANES = 128
VMEM_BYTES = 67043328
MESH = pl.DeviceIdType.MESH
F32 = jnp.float32
BF16 = jnp.bfloat16


def pair_tables(token_length):
    position = np.arange(token_length)
    half_pairs = HEAD_CHANNELS // 4
    inv_freq = (rope_base ** (-np.arange(half_pairs) / half_pairs)).astype(np.float32)
    row = (position // GRID).astype(np.float32)
    col = (position % GRID).astype(np.float32)
    angles = np.concatenate([row[:, None] * inv_freq, col[:, None] * inv_freq], axis=1)
    cos_tab = np.repeat(np.cos(angles), 2, axis=1)
    sin_tab = np.repeat(np.sin(angles), 2, axis=1)
    sin_tab[:, 0::2] *= -1.0
    return (
        np.tile(cos_tab, (1, 2)).astype(np.float32),
        np.tile(sin_tab, (1, 2)).astype(np.float32),
    )


def swap_pairs(x):
    lane = lax.broadcasted_iota(jnp.int32, x.shape, 1)
    return jnp.where(lane % 2 == 0, pltpu.roll(x, LANES - 1, 1), pltpu.roll(x, 1, 1))


def head_mean(z):
    row = lax.broadcasted_iota(jnp.int32, (LANES, LANES), 0) // HEAD_CHANNELS
    col = lax.broadcasted_iota(jnp.int32, (LANES, LANES), 1) // HEAD_CHANNELS
    ones = jnp.where(row == col, 1.0, 0.0).astype(BF16)
    high = z.astype(BF16)
    low = (z - high.astype(F32)).astype(BF16)
    total = jnp.dot(high, ones, preferred_element_type=F32)
    total = total + jnp.dot(low, ones, preferred_element_type=F32)
    return total * (1.0 / HEAD_CHANNELS)


def norm_rotate(x, gain, cos_tab, sin_tab):
    inv = lax.rsqrt(head_mean(x * x) + norm_eps)
    y = x * inv * gain
    return y * cos_tab + swap_pairs(y) * sin_tab, inv


def norm_rotate_back(x, inv, cotangent, gain, cos_tab, sin_tab):
    turned = cotangent * cos_tab - swap_pairs(cotangent) * sin_tab
    weighted = turned * gain
    return inv * (weighted - x * (inv * inv * head_mean(weighted * x)))


def contract(a, b, dims):
    return lax.dot_general(a, b, (dims, ((), ())), preferred_element_type=F32)


def step_kernel(
    n, dp,
    x_hbm, q_hbm, k_hbm, v_hbm, do_hbm, qg_hbm, kg_hbm, km_hbm, vm_hbm, cos_hbm, sin_hbm,
    dx_buf, dq_buf, kw_buf, vw_buf,
    qg_ref, kg_ref, q_buf, do_buf, cos_buf, sin_buf, k_own, v_own, k_head, k_inv, kv_all, q_inv, q_st, do_st,
    x_all, x_t, wk_all, wv_all, dq_acc, part, comb_in, comb, got, g_all, own_k, own_v,
    wg_part, wg_got, fin_all, fin_low,
    ready, local_sem, kv_send, kv_recv, x_sem, w_send, w_recv, p_send, c_recv, p_recv,
    g_send, gd_recv, gm_recv, r_send, r_recv, f_recv,
):
    me = lax.axis_index("sp")
    md = lax.axis_index("dp")
    rows, q_width = q_buf.shape
    heads = kv_all.shape[1]
    share = x_all.shape[2]
    per_group = q_width // (heads * HEAD_CHANNELS)
    half_share = share // 2
    mate = md + 1 - 2 * (md % 2)
    last = n - 1
    first_mid = n // 2 - 1
    partner = me + 1 - 2 * (me % 2)
    low_side = me < n // 2
    other_end = jnp.where(low_side, last, 0)
    other_mid = jnp.where(low_side, n // 2, n // 2 - 1)
    is_end = jnp.logical_or(me == 0, me == last)
    near_chips = dp // 2 - 1
    core = md % 2
    upper = md + 1 - core
    side_mid = jnp.where(is_end, partner, me)
    is_owner = jnp.logical_and(jnp.logical_not(is_end), core == 1)
    first_straight = 0
    relayed = 1

    def sp_peer(o):
        return lax.rem(me + o, n)

    def sp_from(o):
        return lax.rem(me - o + n, n)

    def dp_peer(o):
        return lax.rem(md + o, dp)

    def dp_from(o):
        return lax.rem(md - o + dp, dp)

    def mate_from(o):
        return lax.rem(mate - o + dp, dp)

    def pair(c):
        return pl.ds(c * LANES, LANES)

    def columns(d):
        return pl.ds(pl.multiple_of(d * share, share), share)

    barrier = pltpu.get_barrier_semaphore()

    def greet(where):
        pl.semaphore_signal(barrier, inc=1, device_id=where, device_id_type=MESH)

    @pl.when(me > 0)
    def _():
        greet({"sp": me - 1})

    @pl.when(me < last)
    def _():
        greet({"sp": me + 1})

    @pl.when(jnp.logical_not(is_end))
    def _():
        greet({"sp": other_end})

    def flip(bit):
        return md + bit - 2 * bit * ((md // bit) % 2)

    x_side, y_side = flip(2), flip(4)
    corner = x_side + y_side - md
    beside = [mate]
    for d in (x_side, y_side):
        beside += [d, d + mate - md]
    for d in beside:
        greet({"dp": d})

    my_rows = pl.ds(pl.multiple_of(me * rows, rows), rows)
    wanted = [
        (k_hbm, k_own), (v_hbm, v_own), (cos_hbm.at[my_rows, :], cos_buf),
        (sin_hbm.at[my_rows, :], sin_buf), (kg_hbm, kg_ref), (qg_hbm, qg_ref),
        (q_hbm, q_buf), (do_hbm, do_buf),
        (x_hbm.at[:, columns(md)], x_all.at[md]), (km_hbm, wk_all.at[md]), (vm_hbm, wv_all.at[md]),
    ]
    local = [
        pltpu.make_async_copy(src, dst, local_sem.at[i]) for i, (src, dst) in enumerate(wanted)
    ]
    for copy in local:
        copy.start()

    def remote(src, dst, send, recv, where):
        return pltpu.make_async_remote_copy(
            src_ref=src, dst_ref=dst, send_sem=send, recv_sem=recv,
            device_id=where, device_id_type=MESH,
        )

    def send(*args):
        remote(*args).start()

    def arrived(dst, recv):
        remote(dst, dst, recv, recv, {"sp": me}).wait_recv()

    def departed(src, sem):
        remote(src, src, sem, sem, {"sp": me}).wait_send()

    low_lanes = lax.broadcasted_iota(jnp.int32, (rows, LANES), 1) < HEAD_CHANNELS

    def shift(a):
        return pltpu.roll(a, HEAD_CHANNELS, 1)

    with jax.named_scope("local"):
        for copy in local[:6]:
            copy.wait()
    cos_own = cos_buf[...]
    sin_own = sin_buf[...]
    q_gain = jnp.concatenate([qg_ref[...], qg_ref[...]], axis=1)
    k_gain = jnp.concatenate([kg_ref[...], kg_ref[...]], axis=1)

    for c in range(heads // 2):
        keys = k_own[:, pair(c)].astype(F32)
        vals = v_own[:, pair(c)].astype(F32)
        turned, inv = norm_rotate(keys, k_gain, cos_own, sin_own)
        kv_all[me, 2 * c] = jnp.where(low_lanes, turned, shift(vals)).astype(BF16)
        kv_all[me, 2 * c + 1] = jnp.where(low_lanes, shift(turned), vals).astype(BF16)
        k_head[2 * c] = keys
        k_head[2 * c + 1] = shift(keys)
        k_inv[2 * c] = inv
        k_inv[2 * c + 1] = shift(inv)

    with jax.named_scope("barrier"):
        pl.semaphore_wait(barrier, 2 + len(beside))

    def send_kv(src, g, sem, where):
        block = kv_all.at[src, g]
        send(block, block, kv_send.at[sem], kv_recv.at[src, g], {"sp": where})

    for g in range(heads):
        send_kv(me, g, 0, other_mid)
        send_kv(me, g, 1, partner)

    pl.semaphore_signal(ready, inc=1, device_id={"dp": x_side}, device_id_type=MESH)

    def send_tokens(peers):
        for d in peers:
            send(x_hbm.at[:, columns(d)], x_all.at[md], x_sem.at[0], x_sem.at[1], {"dp": d})

    send_tokens(beside)

    top = pl.ds(0, half_share)
    bottom = pl.ds(half_share, half_share)
    full = pl.ds(0, share)
    weights = [(km_hbm, wk_all, full), (vm_hbm, wv_all, top), (vm_hbm, wv_all, bottom)]

    def send_weights(kind, peers):
        src, dst, at = weights[kind]
        for d in peers:
            send(src.at[at], dst.at[md, at], w_send.at[kind],
                 w_recv.at[kind, 1 if d is mate else 0], {"dp": d})

    def pass_weights(kind):
        _, dst, at = weights[kind]
        arrived(dst.at[pl.ds(0, near_chips), at], w_recv.at[kind, 0])
        for o in range(2, dp, 2):
            block = dst.at[dp_from(o), at]
            send(block, block, w_send.at[kind], w_recv.at[kind, 1], {"dp": mate})

    def finish_weights(kind):
        _, dst, at = weights[kind]
        arrived(dst.at[pl.ds(0, dp // 2), at], w_recv.at[kind, 1])

    for kind in range(2):
        send_weights(kind, (x_side, y_side, mate))

    with jax.named_scope("local2"):
        for copy in local[6:8]:
            copy.wait()
    with jax.named_scope("qrot"):
        for c in range(q_width // LANES):
            turned, inv = norm_rotate(q_buf[:, pair(c)].astype(F32), q_gain, cos_own, sin_own)
            q_inv[:, pair(c)] = inv
            turned = turned * score_scale
            grads = do_buf[:, pair(c)].astype(F32)
            g, r = divmod(2 * c, per_group)
            for a, (query, grad) in enumerate([(turned, shift(grads)), (shift(turned), grads)]):
                to = pl.ds((r + a) * rows, rows)
                q_st[g, to, :] = jnp.where(low_lanes, query, 0.0).astype(BF16)
                do_st[g, to, :] = jnp.where(low_lanes, 0.0, grad).astype(BF16)

    pl.semaphore_wait(ready, 1)
    send_tokens((corner, corner + mate - md))
    for kind in range(2):
        send_weights(kind, (corner,))

    def take_kv(src, g):
        arrived(kv_all.at[src, g], kv_recv.at[src, g])

    def relay(src, g, where):
        take_kv(src, g)
        send_kv(src, g, 2 + src, where)

    def relays(turns):
        @pl.when(jnp.logical_not(is_end))
        def _():
            for src, g in turns:
                relay([other_mid, other_end][src], g, partner)

    turns = sorted(
        [(0, g) for g in range(heads)] + [(1, g) for g in range(heads)],
        key=lambda turn: turn[1] + 0.5 * turn[0],
    )
    with jax.named_scope("relay"):
        relays(turns)

    step = 1

    def attend(g):
        kv = kv_all[:, g].reshape(n * rows, LANES)
        both = None
        score_grads = []
        for r in range(0, per_group, step):
            at = pl.ds(r * rows, step * rows)
            queries = q_st[g, at, :]
            grads = do_st[g, at, :]
            scores = contract(kv, queries, ((1,), (1,)))
            prob_grad = contract(kv, grads, ((1,), (1,)))
            shifted = jnp.exp(scores - jnp.max(scores, axis=0, keepdims=True))
            inverse = 1.0 / jnp.sum(shifted, axis=0, keepdims=True)
            prob = shifted * inverse
            row_dot = jnp.sum(prob * prob_grad, axis=0, keepdims=True)
            score_grad = (prob * (prob_grad - row_dot)).astype(BF16)
            term = contract(score_grad, queries, ((1,), (0,)))
            term = term + contract(prob.astype(BF16), grads, ((1,), (0,)))
            both = term if both is None else both + term
            score_grads.append(score_grad)
        part[g] = both.astype(BF16).reshape(n, rows, LANES)
        return kv, score_grads

    def query_part(g, kv, score_grads):
        parts = [contract(kv[:, :HEAD_CHANNELS], a, ((0,), (0,))) for a in score_grads]
        for r in range(0, per_group, 2):
            head = g * per_group + r
            dq_acc[:, head * HEAD_CHANNELS:head * HEAD_CHANNELS + LANES] = jnp.concatenate(
                [parts[r], parts[r + 1]], axis=0
            ).T

    def straight(g):
        return core == 0 if g >= first_straight else core < 0

    def send_parts(g):
        @pl.when(straight(g))
        def _():
            for where in (other_end, other_mid):
                send(part.at[g, where], got.at[g, jnp.where(is_end, 1, 2)], p_send.at[0],
                     p_recv.at[g], {"sp": where})

        @pl.when(jnp.logical_and(is_end, jnp.logical_not(straight(g))))
        def _():
            for i, where in enumerate([other_end, other_mid]):
                send(part.at[g, where], comb_in.at[g, i], p_send.at[0], c_recv.at[g, i],
                     {"sp": partner})

        send(part.at[g, partner], got.at[g, 0], p_send.at[0], p_recv.at[g], {"sp": partner})

    def combine(g):
        @pl.when(jnp.logical_not(jnp.logical_or(is_end, straight(g))))
        def _():
            for i, where in enumerate([other_end, other_mid]):
                arrived(comb_in.at[g, i], c_recv.at[g, i])
                total = comb_in[g, i].astype(F32) + part[g, where].astype(F32)
                comb[g, i] = total.astype(BF16)
                send(comb.at[g, i], got.at[g, 1], p_send.at[0], p_recv.at[g], {"sp": where})

    def own_grads(g):
        with jax.named_scope(f"gotwait{g}"):
            @pl.when(straight(g))
            def _():
                arrived(got.at[g], p_recv.at[g])

            @pl.when(jnp.logical_not(straight(g)))
            def _():
                arrived(got.at[g, pl.ds(0, 2)], p_recv.at[g])
        total = part[g, me].astype(F32) + got[g, 0].astype(F32) + got[g, 1].astype(F32)
        total = total + jnp.where(straight(g), got[g, 2].astype(F32), 0.0)
        keys = k_head[g]
        back = norm_rotate_back(keys, k_inv[g], total, k_gain, cos_own, sin_own)
        both = jnp.where(low_lanes, back, total).astype(BF16)
        g_all[g, md] = both
        mine = g_all.at[g, md]
        for d in (corner, x_side, y_side):
            send(mine, mine, g_send.at[0], gd_recv.at[g], {"dp": d})
        send(mine, mine, g_send.at[0], gm_recv.at[g], {"dp": mate})
        at = slice(g * HEAD_CHANNELS, (g + 1) * HEAD_CHANNELS)
        own_k[:, at] = both[:, :HEAD_CHANNELS]
        own_v[:, at] = both[:, HEAD_CHANNELS:]

    def pass_on(g):
        with jax.named_scope(f"gdwait{g}"):
            arrived(g_all.at[g, pl.ds(0, near_chips)], gd_recv.at[g])
        for o in range(2, dp, 2):
            block = g_all.at[g, dp_from(o)]
            send(block, block, g_send.at[1], gm_recv.at[g], {"dp": mate})

    def weight_grads(g):
        with jax.named_scope(f"gmwait{g}"):
            arrived(g_all.at[g, pl.ds(0, dp // 2)], gm_recv.at[g])
        total = contract(x_t[...], g_all[g].reshape(dp * rows, LANES), ((1,), (0,)))
        wg_part[g] = total.astype(BF16).reshape(2, half_share, LANES)

        def give(half, where):
            send(wg_part.at[g, half], wg_got.at[g, core * n + me], r_send.at[0],
                 r_recv.at[g, core], {"sp": where, "dp": upper})

        give(other_mid - first_mid, other_mid)

        @pl.when(jnp.logical_not(is_owner))
        def _():
            give(side_mid - first_mid, side_mid)

    def sum_weight_grads(g):
        @pl.when(is_owner)
        def _():
            mine = me - first_mid
            with jax.named_scope(f"rwaits{g}"):
                arrived(wg_got.at[g, pl.ds(0, n)], r_recv.at[g, 0])
            total = wg_got[g, 0].astype(F32)
            for src in range(1, n):
                total = total + wg_got[g, src].astype(F32)
            fin_low[g] = total.astype(BF16)

            def give_out(block, d):
                if g >= relayed:
                    send(block, fin_all.at[g, mine], r_send.at[3], f_recv.at[g],
                         {"sp": other_end, "dp": d})
                for where in (partner, other_mid):
                    send(block, fin_all.at[g, mine], r_send.at[1], f_recv.at[g],
                         {"sp": where, "dp": d})

            give_out(fin_low.at[g], mate)
            with jax.named_scope(f"rwait{g}"):
                arrived(wg_got.at[g, pl.ds(0, last)], r_recv.at[g, 1])
            total = wg_part[g, mine].astype(F32)
            for o in range(1, n):
                total = total + wg_got[g, n + sp_from(o)].astype(F32)
            fin_all[g, mine] = total.astype(BF16)
            give_out(fin_all.at[g, mine], md)
            send(fin_low.at[g], fin_all.at[g, mine], r_send.at[1], f_recv.at[g], {"dp": mate})

    def hand_on(g):
        block = fin_all.at[g, other_mid - first_mid]
        send(block, block, r_send.at[2], f_recv.at[g], {"sp": partner})

    def relay_weight_grads(g):
        @pl.when(is_owner)
        def _():
            arrived(fin_all.at[g, 0], f_recv.at[g])
            hand_on(g)

    def put_weight_grads(g):
        with jax.named_scope(f"fwait{g}"):
            if g >= relayed:
                @pl.when(is_owner)
                def _():
                    arrived(fin_all.at[g, 0], f_recv.at[g])

            @pl.when(jnp.logical_not(is_owner))
            def _():
                arrived(fin_all.at[g], f_recv.at[g])
        if g < relayed:
            @pl.when(jnp.logical_not(jnp.logical_or(is_end, is_owner)))
            def _():
                hand_on(g)
        total = fin_all[g].reshape(share, LANES).astype(F32)
        at = slice(g * HEAD_CHANNELS, (g + 1) * HEAD_CHANNELS)
        kw_buf[:, at] = total[:, :HEAD_CHANNELS]
        vw_buf[:, at] = total[:, HEAD_CHANNELS:]

    def query_grads(c):
        dq_buf[:, pair(c)] = norm_rotate_back(
            q_buf[:, pair(c)].astype(F32), q_inv[:, pair(c)], dq_acc[:, pair(c)],
            q_gain * score_scale, cos_own, sin_own,
        ).astype(BF16)

    def project(src):
        out = contract(own_k[...], wk_all[src], ((1,), (1,)))
        out = out + contract(own_v[...], wv_all[src], ((1,), (1,)))
        dx_buf[:, columns(src)] = out.astype(BF16)

    blocks = q_width // LANES
    for g in range(heads):
        with jax.named_scope(f"kvwait{g}"):
            take_kv(partner, g)

            @pl.when(is_end)
            def _():
                take_kv(other_mid, g)
                take_kv(other_end, g)
        if g == heads - 1:
            with jax.named_scope("comb0"):
                combine(0)
        with jax.named_scope(f"attend{g}"):
            kept = attend(g)
            send_parts(g)
            query_part(g, *kept)
    def scoped(name, step, *args):
        with jax.named_scope(name):
            step(*args)

    def query_half(first):
        for c in range(first, first + blocks // 2):
            query_grads(c)

    scoped("comb1", combine, 1)
    scoped("comb2", combine, 2)
    scoped("comb3", combine, 3)
    scoped("dqa", query_half, 0)
    scoped("own0", own_grads, 0)
    scoped("own1", own_grads, 1)
    with jax.named_scope("xt"):
        for copy in local[8:]:
            copy.wait()
        arrived(x_all.at[pl.ds(0, dp - 1)], x_sem.at[1])
        for src in range(dp):
            x_t[:, src * rows:(src + 1) * rows] = x_all[src].T
    scoped("own2", own_grads, 2)
    scoped("pass0", pass_on, 0)
    scoped("own3", own_grads, 3)
    send_weights(2, (x_side, y_side, corner, mate))
    scoped("dqb", query_half, blocks // 2)
    with jax.named_scope("wpass"):
        pass_weights(0)
        pass_weights(1)
    scoped("wg0", weight_grads, 0)
    scoped("pass1", pass_on, 1)
    scoped("wg1", weight_grads, 1)
    scoped("pass2", pass_on, 2)
    scoped("pass3", pass_on, 3)
    scoped("sum0", sum_weight_grads, 0)
    scoped("wg2", weight_grads, 2)
    scoped("wg3", weight_grads, 3)
    scoped("sum1", sum_weight_grads, 1)
    scoped("wlate", pass_weights, 2)
    with jax.named_scope("proja"):
        for o in range(0, dp, 2):
            project(dp_from(o))
    scoped("hand0", relay_weight_grads, 0)
    scoped("sum2", sum_weight_grads, 2)
    scoped("sum3", sum_weight_grads, 3)
    with jax.named_scope("wfin"):
        for kind in range(3):
            finish_weights(kind)
    with jax.named_scope("projb"):
        for o in range(0, dp, 2):
            project(mate_from(o))
    for g in range(heads):
        scoped(f"put{g}", put_weight_grads, g)

    with jax.named_scope("drain"):
        departed(kv_all.at[me], kv_send.at[0])
        departed(kv_all.at[me], kv_send.at[1])

        @pl.when(jnp.logical_not(is_end))
        def _():
            departed(kv_all.at[other_mid], kv_send.at[2 + other_mid])
            departed(kv_all.at[other_end], kv_send.at[2 + other_end])

        departed(x_all.at[pl.ds(0, dp - 1)], x_sem.at[0])
        for kind, (_, dst, at) in enumerate(weights):
            departed(dst.at[pl.ds(0, dp - 1), at], w_send.at[kind])
        departed(part.at[:, pl.ds(0, 3)], p_send.at[0])
        departed(g_all.at[:, pl.ds(0, dp // 2)], g_send.at[0])
        departed(g_all.at[:, pl.ds(0, near_chips)], g_send.at[1])

        @pl.when(is_owner)
        def _():
            departed(wg_part.at[:, 0], r_send.at[0])
            departed(wg_got.at[:, pl.ds(0, 5)], r_send.at[1])
            departed(wg_got.at[pl.ds(0, heads - relayed), pl.ds(0, 2)], r_send.at[3])

        @pl.when(jnp.logical_not(is_owner))
        def _():
            departed(wg_part, r_send.at[0])

        @pl.when(jnp.logical_not(is_end))
        def _():
            departed(fin_low.at[pl.ds(0, relayed)], r_send.at[2])


def write_kernel(*refs):
    count = (len(refs) - 1) // 2
    copies = [
        pltpu.make_async_copy(refs[i], refs[count + i], refs[-1].at[i]) for i in range(count)
    ]
    for copy in copies:
        copy.start()
    for copy in copies:
        copy.wait()


def kernel_step(
    n, dp, inputs, queries, keys, values, out_grad, query_gain, key_gain, key_matrix, value_matrix
):
    rows, width = inputs.shape[1:]
    q_width = queries.shape[2]
    kv_width = keys.shape[2]
    length = rows * n
    share = width // dp
    kv_heads = kv_width // HEAD_CHANNELS
    stack = rows * (q_width // kv_width)
    cos_tab, sin_tab = pair_tables(length)
    vmem = pltpu.VMEM
    dma = pltpu.SemaphoreType.DMA
    packed = (rows, LANES)
    scratch = [
        vmem((1, HEAD_CHANNELS), F32), vmem((1, HEAD_CHANNELS), F32),
        vmem((rows, q_width), BF16), vmem((rows, q_width), BF16),
        vmem(packed, F32), vmem(packed, F32),
        vmem((rows, kv_width), BF16), vmem((rows, kv_width), BF16),
        vmem((kv_heads, *packed), F32), vmem((kv_heads, *packed), F32),
        vmem((n, kv_heads, *packed), BF16),
        vmem((rows, q_width), F32),
        vmem((kv_heads, stack, LANES), BF16), vmem((kv_heads, stack, LANES), BF16),
        vmem((dp, rows, share), BF16), vmem((share, dp * rows), BF16),
        vmem((dp, share, kv_width), BF16), vmem((dp, share, kv_width), BF16),
        vmem((rows, q_width), F32),
        vmem((kv_heads, n, *packed), BF16),
        vmem((kv_heads, 2, *packed), BF16), vmem((kv_heads, 2, *packed), BF16),
        vmem((kv_heads, 3, *packed), BF16),
        vmem((kv_heads, dp, *packed), BF16),
        vmem((rows, kv_width), BF16), vmem((rows, kv_width), BF16),
        vmem((kv_heads, 2, share // 2, LANES), BF16),
        vmem((kv_heads, 2 * n, share // 2, LANES), BF16),
        vmem((kv_heads, 2, share // 2, LANES), BF16), vmem((kv_heads, share // 2, LANES), BF16),
        pltpu.SemaphoreType.REGULAR, dma((11,)), dma((2 + n,)), dma((n, kv_heads)), dma((2,)), dma((3,)), dma((3, 2)),
        dma((1,)), dma((kv_heads, 2)), dma((kv_heads,)),
        dma((2,)), dma((kv_heads,)), dma((kv_heads,)),
        dma((4,)), dma((kv_heads, 2)), dma((kv_heads,)),
    ]
    hbm = pl.BlockSpec(memory_space=pltpu.HBM)
    here = pl.BlockSpec(memory_space=pltpu.VMEM)
    results = [
        ((rows, width), BF16), ((rows, q_width), BF16),
        ((share, kv_width), F32), ((share, kv_width), F32),
    ]
    held_bytes = 65536 + sum(a * b * jnp.dtype(kind).itemsize for (a, b), kind in results)
    held = pl.pallas_call(
        functools.partial(step_kernel, n, dp),
        out_shape=[pltpu.VMEM(shape, kind) for shape, kind in results],
        in_specs=[hbm] * 11,
        out_specs=[here] * 4,
        scratch_shapes=scratch,
        compiler_params=pltpu.CompilerParams(
            collective_id=0, has_side_effects=True, vmem_limit_bytes=VMEM_BYTES - held_bytes
        ),
    )(
        inputs[0], queries[0], keys[0], values[0], out_grad[0],
        query_gain[None], key_gain[None],
        key_matrix, value_matrix, jnp.asarray(cos_tab), jnp.asarray(sin_tab),
    )
    dx, dq, kw, vw = pl.pallas_call(
        write_kernel,
        out_shape=[jax.ShapeDtypeStruct(shape, kind) for shape, kind in results],
        in_specs=[here] * 4,
        out_specs=[hbm] * 4,
        scratch_shapes=[dma((4,))],
        compiler_params=pltpu.CompilerParams(vmem_limit_bytes=8 * 1024 * 1024),
    )(*held)
    return dx[None], dq[None], kw, vw


def device_step(inputs, *rest):
    n = lax.axis_size("sp")
    dp = lax.axis_size("dp")
    rows, width = inputs.shape[1:]
    fits = n == 4 and dp == 8 and width % (dp * LANES) == 0 and rows == LANES
    if fits and (width // dp) % (32 * n) == 0:
        return kernel_step(n, dp, inputs, *rest)
    return on_device(inputs, *rest)


def solution(mesh):
    return jax.shard_map(
        device_step,
        mesh=mesh,
        in_specs=(
            P("dp", "sp", None),
            P("dp", "sp", None),
            P("dp", "sp", None),
            P("dp", "sp", None),
            P("dp", "sp", None),
            P(),
            P(),
            P("dp", None),
            P("dp", None),
        ),
        out_specs=(P("dp", "sp", None), P("dp", "sp", None), P("dp", None), P("dp", None)),
        check_vma=False,
    )
```
